32 devices in a mesh: ep: 8 (over z, x), tp: 4 (over y, core).
Axes of the slice: x: 2, y: 2, z: 4, core: 2. Of those that a mesh axis runs over, the one named last changes fastest.
Arguments:
- tokens: bfloat16 [64, 1024], P('ep'), may hold values from -6 to 6
- kv_cache: bfloat16 [64, 4, 1024, 128], P('ep', 'tp'), may hold values from -6 to 6
- lengths: int32 [64], P('ep'), may hold values from 256 to 1024
- w_query: bfloat16 [1024, 512], P(None, 'tp'), may hold values from -0.1875 to 0.1875
- w_key: bfloat16 [1024, 256], P(None, 'tp'), may hold values from -0.1875 to 0.1875
- w_value: bfloat16 [1024, 256], P(None, 'tp'), may hold values from -0.1875 to 0.1875
- break_bias: float32 [8], P('tp'), may hold values from -7.5 to -3.5
- head_gain: float32 [512], P('tp'), may hold values from 0.1 to 1.9
- w_output: bfloat16 [512, 1024], P('tp'), may hold values from -0.25 to 0.25
- attn_norm_gain: float32 [1024], replicated, may hold values from 0.1 to 1.9
- w_router: bfloat16 [1024, 16], replicated, may hold values from -0.1875 to 0.1875
- routes: int32 [64, 2], P('ep'), may hold values from 0 to 15, all different within a row; in each aligned block of 8 rows (0 to 7, 8 to 15, ...) at most 2 rows name the same one
- expert_gate: bfloat16 [1024, 57344], P(None, ('ep', 'tp')), may hold values from -0.1875 to 0.1875
- expert_up: bfloat16 [1024, 57344], P(None, ('ep', 'tp')), may hold values from -0.1875 to 0.1875
- expert_down: bfloat16 [57344, 1024], P(('ep', 'tp')), may hold values from -0.09375 to 0.09375
- dense_gate: bfloat16 [1024, 2816], P(None, 'ep'), may hold values from -0.1875 to 0.1875
- dense_up: bfloat16 [1024, 2816], P(None, 'ep'), may hold values from -0.1875 to 0.1875
- dense_down: bfloat16 [2816, 1024], P('ep', 'tp'), may hold values from -0.109375 to 0.109375
- mix_gate: bfloat16 [1024], replicated, may hold values from -0.1875 to 0.1875
- ffn_norm_gain: float32 [1024], P('tp'), may hold values from 0.1 to 1.9
Outputs:
- layer_out: bfloat16 [64, 1024], P('ep', 'tp')
- new_kv: bfloat16 [64, 4, 128], P('ep', 'tp')
The draws below stay inside these ranges and needn't reach their ends.
Inputs may be any that keep to these rules, and one draw needn't show every extreme that they name: lengths[b] is the number of valid cached positions of sequence b and the new token's position. `routes`: each row names 2 different experts. Among the rows of one index of ep (aligned blocks of 8 rows) no expert is named more than 2 times, a bound that some block reaches.
All inputs are finite; a program needn't handle non-finite values.
Results may differ from the reference program's by a relative error of at most 0.012.
Values may be sent and summed in bfloat16 or wider, within the bound.
A program may use at most 128 MiB of HBM per device.

```python
import math
import jax
import jax.numpy as jnp
import numpy as np
from jax import lax

D = 1024
H = 8
KV = 4
HD = 64
L = 1024
SEQ_DEV = 8
EXPERTS = 16
TOPK = 2
FE = 3584
FFD = 2816
CAP = 2
SEQS = 64


def touch_ends(array, rng, low, largest):
    shape = array.shape
    spot = [jax.random.randint(jax.random.fold_in(rng, axis), (), 0, shape[axis]) for axis in range(len(shape))]
    array = array.at[tuple(spot)].set(low)
    longest = shape.index(max(shape))
    spot[longest] = (spot[longest] + 1) % shape[longest]
    return array.at[tuple(spot)].set(largest)


def shard_levels(stream_key, dims, cuts, smallest, top_value):
    level = 1.0
    for dim, shards_of in cuts:
        draws = jax.random.uniform(jax.random.fold_in(jax.random.fold_in(stream_key, 6), dim), (shards_of,), jnp.float32, smallest / len(cuts), top_value / len(cuts))
        level = level * jnp.repeat(jnp.exp(draws), dims[dim] // shards_of).reshape((-1,) + (1,) * (len(dims) - 1 - dim))
    return level


def assign_block(rng, own, number, rows, amount, top, reach, skew):
    ranking = jax.random.permutation(rng, amount)
    crowded, ordinary = load_shares(amount, rows * top, reach, skew, True), load_shares(amount, rows * top, reach, skew, False)
    places = jnp.arange(amount)

    def named(sizes, rotation):
        used = int((sizes > 0).sum())
        fixed = max(1, used // 4)
        moved = fixed + (places - fixed + rotation * (used - fixed)) % max(1, amount - fixed)
        return jnp.zeros((amount,), jnp.int32).at[ranking[jnp.where(places < fixed, places, moved)]].set(jnp.asarray(sizes, jnp.int32))

    sizes = jnp.where(number % 4 == 0, named(crowded, number // 4), named(ordinary, number - number // 4 - 1))
    mixed = jax.random.permutation(jax.random.fold_in(own, 3), amount)
    donor, sink = mixed[0:amount // 2 * 2:2], mixed[1:amount // 2 * 2:2]
    slack = jnp.minimum(sizes[donor] - 1, reach - sizes[sink]) // 2
    slack = jnp.where((donor == ranking[0]) | (sink == ranking[0]) | (sizes[sink] == 0), 0, jnp.maximum(slack, 0))
    moved = jax.random.randint(jax.random.fold_in(own, 4), (amount // 2,), 0, 1 << 20) % (slack + 1)
    sizes = sizes.at[donor].add(-moved).at[sink].add(moved)
    members = jnp.searchsorted(jnp.cumsum(sizes), jnp.arange(rows * top), side="right").astype(jnp.int32)
    listing = members.reshape(top, rows).T
    listing = listing[jax.random.permutation(jax.random.fold_in(own, 1), rows)]
    rotation = jax.random.randint(jax.random.fold_in(own, 2), (rows, 1), 0, top)
    return jnp.take_along_axis(listing, (jnp.arange(top)[None, :] + rotation) % top, axis=1)


def load_shares(count, total, limit, lean, full):
    loads = [(1 << 20) // math.isqrt(rank ** lean) + 1 for rank in range(1, count + 1)]
    largest = limit if full else min(limit, max(-(-total // count), total * loads[0] // sum(loads)))
    least = 1 if total - largest >= count - 1 else 0
    counts, surplus = [largest] + [least] * (count - 1), total - largest - least * (count - 1)
    while surplus > 0:
        free = [i for i in range(1, count) if counts[i] < largest] or [i for i in range(1, count) if counts[i] < limit]
        whole, left = sum([loads[i] for i in free]), surplus
        for i in free:
            addition = min(limit - counts[i], max(1, left * loads[i] // whole), surplus)
            counts[i] = counts[i] + addition
            surplus = surplus - addition
    return np.array(counts)


def normal_values(key, extent, scale, reach, pieces=(), kind=jnp.bfloat16):
    array = jax.random.normal(key, extent, jnp.float32) * scale
    if len(pieces) > 0:
        array = shard_levels(key, extent, pieces, -0.22, 0.18) * array
    return jnp.clip(array, min=-reach, max=reach).astype(kind)


def setup_inputs(seed: int = 0) -> dict:
    key_list = jax.random.split(jax.random.key(seed), 21)
    tokens = normal_values(key_list[0], (SEQS, D), 1.0, 6.0, ((0, 8),))
    kv_cache = normal_values(key_list[1], (SEQS, KV, L, 2 * HD), 1.0, 6.0, ((0, 8), (1, 4)))
    lengths = touch_ends(jax.random.randint(key_list[2], (SEQS,), L // 4, L + 1), jax.random.fold_in(key_list[2], 1), L // 4, L).astype(jnp.int32)
    w_query = normal_values(key_list[3], (D, H * HD), D ** -0.5, 0.1875, ((1, 4),))
    w_key = normal_values(key_list[4], (D, KV * HD), D ** -0.5, 0.1875, ((1, 4),))
    w_value = normal_values(key_list[5], (D, KV * HD), D ** -0.5, 0.1875, ((1, 4),))
    break_bias = jnp.clip(-7.5 + 4.0 * jax.random.uniform(key_list[6], (H,), jnp.float32) ** shard_levels(key_list[6], (H,), ((0, 4),), -0.2, 0.2), -7.5, -3.5)
    head_gain = jnp.clip(1.0 + 0.18 * jax.random.normal(key_list[7], (H * HD,), jnp.float32), 0.1, 1.9)
    w_output = normal_values(key_list[8], (H * HD, D), (H * HD) ** -0.5, 0.25, ((0, 4),))
    attn_norm_gain = jnp.clip(1.0 + 0.18 * jax.random.normal(key_list[9], (D,), jnp.float32), 0.1, 1.9)
    w_router = normal_values(key_list[10], (D, EXPERTS), D ** -0.5, 0.1875)
    routes_keys = jax.random.split(jax.random.fold_in(key_list[11], 1), SEQS // SEQ_DEV)
    routes_turns = jax.random.permutation(jax.random.fold_in(key_list[11], 3), SEQS // SEQ_DEV)
    routes = jax.vmap(lambda own, number: assign_block(jax.random.fold_in(key_list[11], 2), own, number, SEQ_DEV, EXPERTS, TOPK, CAP, 2))(routes_keys, routes_turns).reshape((SEQS, TOPK))
    expert_gate = normal_values(key_list[12], (D, EXPERTS * FE), D ** -0.5, 0.1875, ((1, 32),))
    expert_up = normal_values(key_list[13], (D, EXPERTS * FE), D ** -0.5, 0.1875, ((1, 32),))
    expert_down = normal_values(key_list[14], (EXPERTS * FE, D), FE ** -0.5, 0.09375, ((0, 32),))
    dense_gate = normal_values(key_list[15], (D, FFD), D ** -0.5, 0.1875, ((1, 8),))
    dense_up = normal_values(key_list[16], (D, FFD), D ** -0.5, 0.1875, ((1, 8),))
    dense_down = normal_values(key_list[17], (FFD, D), FFD ** -0.5, 0.109375, ((0, 8), (1, 4)))
    mix_gate = normal_values(key_list[18], (D,), D ** -0.5, 0.1875)
    ffn_norm_gain = jnp.clip(1.0 + 0.18 * jax.random.normal(key_list[19], (D,), jnp.float32), 0.1, 1.9)
    return dict(tokens=tokens, kv_cache=kv_cache, lengths=lengths, w_query=w_query, w_key=w_key, w_value=w_value, break_bias=break_bias, head_gain=head_gain, w_output=w_output, attn_norm_gain=attn_norm_gain, w_router=w_router, routes=routes, expert_gate=expert_gate, expert_up=expert_up, expert_down=expert_down, dense_gate=dense_gate, dense_up=dense_up, dense_down=dense_down, mix_gate=mix_gate, ffn_norm_gain=ffn_norm_gain)


RESIDUAL_SCALE = 8.0 ** 0.25

def layer_norm(values, gain):
    centre = lax.optimization_barrier(jnp.mean(values, axis=-1, keepdims=True))
    centred = values - centre
    spread = lax.optimization_barrier(jnp.mean(centred * centred, axis=-1, keepdims=True))
    return centred * lax.rsqrt(spread + 1e-05) * gain

def reference(tokens, kv_cache, lengths, w_query, w_key, w_value, break_bias, head_gain, w_output, attn_norm_gain, w_router, routes, expert_gate, expert_up, expert_down, dense_gate, dense_up, dense_down, mix_gate, ffn_norm_gain):
    seq_count = tokens.shape[0]
    group_size = H // KV
    blocks = seq_count // SEQ_DEV
    queries = jnp.dot(tokens, w_query, preferred_element_type=jnp.float32).astype(jnp.bfloat16)
    key_new = jnp.dot(tokens, w_key, preferred_element_type=jnp.float32).astype(jnp.bfloat16).reshape(seq_count, KV, HD)
    value_new = jnp.dot(tokens, w_value, preferred_element_type=jnp.float32).astype(jnp.bfloat16).reshape(seq_count, KV, HD)
    new_kv = jnp.concatenate([key_new, value_new], axis=2)
    bias_grid = break_bias.reshape(1, KV, group_size, 1)

    def attend(block_args):
        query_block, cache_block, length = block_args
        query_wide = query_block.reshape(-1, KV, group_size, HD).astype(jnp.float32)
        cached_keys = cache_block[..., :HD].astype(jnp.float32)
        value_rows = cache_block[..., HD:].astype(jnp.float32)
        scores = jnp.einsum('bgqd,bgld->bgql', query_wide, cached_keys) * HD ** (-0.5) + bias_grid
        visible = jnp.arange(L, dtype=jnp.int32)[None, None, None, :] < length[:, None, None, None]
        survive = jnp.where(visible, jax.nn.log_sigmoid(-scores), 0.0)
        remaining = lax.cumsum(survive, axis=3, reverse=True) - survive
        weights = jnp.where(visible, jnp.exp(jax.nn.log_sigmoid(scores) + remaining), 0.0).astype(jnp.bfloat16)
        blended = jnp.einsum('bgql,bgld->bgqd', weights.astype(jnp.float32), value_rows)
        rescale = lax.rsqrt(lax.optimization_barrier(jnp.mean(blended * blended, axis=3, keepdims=True)) + 1e-06)
        return ((blended * rescale).reshape(-1, H * HD) * head_gain).astype(jnp.bfloat16)
    normed = lax.map(attend, (queries.reshape(blocks, SEQ_DEV, H * HD), kv_cache.reshape(blocks, SEQ_DEV, KV, L, 2 * HD), lengths.reshape(blocks, SEQ_DEV)))
    normed = normed.reshape(seq_count, H * HD)
    attended = jnp.dot(normed, w_output, preferred_element_type=jnp.float32)
    settled = layer_norm(RESIDUAL_SCALE * tokens.astype(jnp.float32) + attended, attn_norm_gain).astype(jnp.bfloat16)
    logits = jnp.dot(settled, w_router, preferred_element_type=jnp.float32)
    picked = jnp.take_along_axis(logits, routes, axis=1)
    route_weight = jax.nn.sigmoid(picked - picked[:, ::-1])
    block_routes = routes.reshape(blocks, SEQ_DEV * TOPK)
    assigned = (block_routes[:, :, None] == jnp.arange(EXPERTS, dtype=jnp.int32)[None, None, :]).astype(jnp.int32)
    before = (jnp.cumsum(assigned, axis=1) - assigned).astype(jnp.int32)
    slot_index = lax.optimization_barrier(jnp.sum(before * assigned, axis=2)).astype(jnp.int32)
    position = (jnp.arange(blocks, dtype=jnp.int32)[:, None] * CAP + slot_index).reshape(-1).astype(jnp.int32)
    expert_flat = routes.reshape(-1).astype(jnp.int32)
    token_flat = jnp.repeat(jnp.arange(seq_count, dtype=jnp.int32), TOPK)
    slot_table = jnp.zeros((EXPERTS, blocks * CAP), jnp.int32).at[expert_flat, position].set(token_flat)
    gate_stack = expert_gate.reshape(D, EXPERTS, FE).transpose(1, 0, 2)
    up_stack = expert_up.reshape(D, EXPERTS, FE).transpose(1, 0, 2)
    down_stack = expert_down.reshape(EXPERTS, FE, D)

    def serve_rows(block_args):
        row_index, gate_weight, up_weight, down_weight = block_args
        received = settled[row_index]
        gate_pre = jnp.dot(received, gate_weight, preferred_element_type=jnp.float32)
        up_pre = jnp.dot(received, up_weight, preferred_element_type=jnp.float32)
        hidden = (jax.nn.silu(gate_pre) * up_pre).astype(jnp.bfloat16)
        return jnp.dot(hidden, down_weight, preferred_element_type=jnp.float32)
    served = lax.map(serve_rows, (slot_table, gate_stack, up_stack, down_stack))
    picked_rows = served[expert_flat, position].reshape(seq_count, TOPK, D)
    routed = lax.optimization_barrier(jnp.sum(picked_rows * route_weight[:, :, None], axis=1))
    dense_gate_pre = jnp.dot(settled, dense_gate, preferred_element_type=jnp.float32)
    dense_up_pre = jnp.dot(settled, dense_up, preferred_element_type=jnp.float32)
    dense_hidden = (jax.nn.silu(dense_gate_pre) * dense_up_pre).astype(jnp.bfloat16)
    dense_out = jnp.dot(dense_hidden, dense_down, preferred_element_type=jnp.float32)
    mix_weight = jax.nn.sigmoid(jnp.dot(settled, mix_gate, preferred_element_type=jnp.float32))
    combined = RESIDUAL_SCALE * settled.astype(jnp.float32) + routed + mix_weight[:, None] * dense_out
    return (layer_norm(combined, ffn_norm_gain).astype(jnp.bfloat16), new_kv)
```

```python
import functools

import jax
import jax.numpy as jnp
from jax import lax
from jax.experimental import pallas as pl
from jax.experimental.pallas import tpu as pltpu
from jax.sharding import PartitionSpec as P

FE = 3584
CAP = 2


RESIDUAL_SCALE = 8.0**0.25
PRECISE = lax.Precision.HIGHEST


def layer_norm(values, gain):
    centre = jnp.mean(values, axis=-1, keepdims=True)
    centred = values - centre
    spread = jnp.mean(centred * centred, axis=-1, keepdims=True)
    return centred * lax.rsqrt(spread + 1e-05) * gain


def stick_weights(scores, visible):
    survive = jnp.where(visible, jax.nn.log_sigmoid(-scores), 0.0)
    remaining = lax.cumsum(survive, axis=3, reverse=True) - survive
    return jnp.where(visible, jnp.exp(jax.nn.log_sigmoid(scores) + remaining), 0.0)


def body(
    tokens,
    kv_cache,
    lengths,
    w_query,
    w_key,
    w_value,
    break_bias,
    head_gain,
    w_output,
    attn_norm_gain,
    w_router,
    routes,
    expert_gate,
    expert_up,
    expert_down,
    dense_gate,
    dense_up,
    dense_down,
    mix_gate,
    ffn_norm_gain,
):
    seq_count = tokens.shape[0]
    model_width = tokens.shape[1]
    key_heads = kv_cache.shape[1]
    positions = kv_cache.shape[2]
    head_dim = kv_cache.shape[3] // 2
    local_heads = w_query.shape[1] // head_dim
    group_size = local_heads // key_heads
    queries = jnp.dot(tokens, w_query, preferred_element_type=jnp.float32).astype(jnp.bfloat16)
    queries = queries.reshape(seq_count, key_heads, group_size, head_dim)
    key_new = jnp.dot(tokens, w_key, preferred_element_type=jnp.float32).astype(jnp.bfloat16)
    value_new = jnp.dot(tokens, w_value, preferred_element_type=jnp.float32).astype(jnp.bfloat16)
    new_kv = jnp.concatenate(
        [
            key_new.reshape(seq_count, key_heads, head_dim),
            value_new.reshape(seq_count, key_heads, head_dim),
        ],
        axis=2,
    )
    cached_keys = kv_cache[..., :head_dim]
    cached_values = kv_cache[..., head_dim:]
    scores = jnp.einsum(
        "bgqd,bgld->bgql", queries, cached_keys, preferred_element_type=jnp.float32
    ) * head_dim ** (-0.5)
    scores = scores + break_bias.reshape(1, key_heads, group_size, 1)
    visible = lax.broadcasted_iota(jnp.int32, (seq_count, 1, 1, positions), 3) < lengths.reshape(
        seq_count, 1, 1, 1
    )
    weights = stick_weights(scores, visible).astype(jnp.bfloat16)
    blended = jnp.einsum(
        "bgql,bgld->bgqd", weights, cached_values, preferred_element_type=jnp.float32
    )
    rescale = lax.rsqrt(jnp.mean(blended * blended, axis=3, keepdims=True) + 1e-06)
    normed = ((blended * rescale).reshape(seq_count, local_heads * head_dim) * head_gain).astype(
        jnp.bfloat16
    )
    partial_out = jnp.dot(normed, w_output, preferred_element_type=jnp.float32)
    attended = lax.psum(partial_out.astype(jnp.bfloat16), "tp").astype(jnp.float32)
    settled = layer_norm(
        RESIDUAL_SCALE * tokens.astype(jnp.float32) + attended, attn_norm_gain
    ).astype(jnp.bfloat16)
    experts = w_router.shape[1]
    top_count = routes.shape[1]
    logits = jnp.dot(settled, w_router, preferred_element_type=jnp.float32)
    chosen = routes[:, :, None] == lax.broadcasted_iota(
        jnp.int32, (seq_count, top_count, experts), 2
    )
    picked = jnp.sum(jnp.where(chosen, logits[:, None, :], 0.0), axis=2)
    route_weight = jax.nn.sigmoid(picked - picked[:, ::-1])
    assigned = chosen.reshape(seq_count * top_count, experts).astype(jnp.int32)
    before = jnp.cumsum(assigned, axis=0) - assigned
    slot_index = jnp.sum(before * assigned, axis=1)
    slot_hits = (
        slot_index[:, None] == lax.broadcasted_iota(jnp.int32, (seq_count * top_count, CAP), 1)
    ).astype(jnp.int32)
    placement = (assigned[:, :, None] * slot_hits[:, None, :]).reshape(
        seq_count, top_count, experts * CAP
    )
    selector = jnp.sum(placement, axis=1).astype(jnp.bfloat16)
    weighted = jnp.sum(placement.astype(jnp.float32) * route_weight[:, :, None], axis=1)
    buffer = lax.dot_general(
        selector, settled, (((0,), (0,)), ((), ())), preferred_element_type=jnp.float32
    )
    buffer = buffer.astype(jnp.bfloat16).reshape(experts, CAP, model_width)
    hosts = lax.axis_size("ep")
    tp_size = lax.axis_size("tp")
    if experts >= hosts:
        per_host = experts // hosts
        outgoing = buffer.reshape(hosts, per_host, CAP, model_width)
    else:
        per_host = 1
        outgoing = jnp.repeat(buffer, hosts // experts, axis=0).reshape(hosts, 1, CAP, model_width)
    columns = expert_gate.shape[1]
    block_index = lax.axis_index(("ep", "tp"))
    own_expert = block_index * columns // FE
    local_slot = own_expert - lax.axis_index("ep") * experts // hosts
    slice_width = model_width // tp_size
    arrived = lax.all_to_all(outgoing, "ep", split_axis=0, concat_axis=0, tiled=True)
    slot_count = arrived.shape[2]
    received = lax.dynamic_index_in_dim(arrived, local_slot, 1, keepdims=False)
    received = received.reshape(hosts * slot_count, model_width)
    gate_pre = jnp.dot(received, expert_gate, preferred_element_type=jnp.float32)
    up_pre = jnp.dot(received, expert_up, preferred_element_type=jnp.float32)
    hidden = (jax.nn.silu(gate_pre) * up_pre).astype(jnp.bfloat16)
    partial_value = jnp.dot(hidden, expert_down, preferred_element_type=jnp.float32)
    partial_value = partial_value.reshape(hosts, 1, slot_count, model_width)
    slot_mask = (lax.broadcasted_iota(jnp.int32, (1, per_host, 1, 1), 1) == local_slot).astype(
        jnp.float32
    )
    summed = lax.psum_scatter(
        (partial_value * slot_mask).astype(jnp.bfloat16), "tp", scatter_dimension=3, tiled=True
    ).astype(jnp.float32)
    returned = lax.all_to_all(
        summed.astype(jnp.bfloat16), "ep", split_axis=0, concat_axis=0, tiled=True
    ).astype(summed.dtype)
    host_ids = lax.broadcasted_iota(jnp.int32, (hosts * per_host,), 0)
    host_expert = host_ids // per_host * experts // hosts + host_ids % per_host
    ownership = (
        host_expert[None, :] == lax.broadcasted_iota(jnp.int32, (experts, hosts * per_host), 0)
    ).astype(jnp.float32)
    gathered = jnp.dot(
        ownership, returned.reshape(hosts * per_host, CAP * slice_width), precision=PRECISE
    )
    gathered = gathered.reshape(experts * CAP, slice_width)
    routed = jnp.dot(weighted, gathered, precision=PRECISE)
    column_rank = lax.axis_index("tp")
    own_settled = lax.dynamic_slice_in_dim(settled, column_rank * slice_width, slice_width, 1)
    shard_rows = lax.all_gather(settled, "ep", axis=0, tiled=True)
    gate_pre = jnp.dot(shard_rows, dense_gate, preferred_element_type=jnp.float32)
    up_pre = jnp.dot(shard_rows, dense_up, preferred_element_type=jnp.float32)
    dense_hidden = (jax.nn.silu(gate_pre) * up_pre).astype(jnp.bfloat16)
    own_hidden = lax.all_to_all(dense_hidden, "ep", split_axis=0, concat_axis=1, tiled=True)
    dense_out = jnp.dot(
        own_hidden,
        lax.all_gather(dense_down, "ep", axis=0, tiled=True),
        preferred_element_type=jnp.float32,
    )
    mix_weight = jax.nn.sigmoid(jnp.dot(settled, mix_gate, preferred_element_type=jnp.float32))
    combined = (
        RESIDUAL_SCALE * own_settled.astype(jnp.float32) + routed + mix_weight[:, None] * dense_out
    )
    row_sums, squares = lax.psum(
        (jnp.sum(combined, axis=1), jnp.sum(combined * combined, axis=1)), "tp"
    )
    row_mean = row_sums / model_width
    row_var = squares / model_width - row_mean * row_mean
    result = (
        (combined - row_mean[:, None]) * lax.rsqrt(row_var[:, None] + 1e-05) * ffn_norm_gain
    ).astype(jnp.bfloat16)
    return (result, new_kv)


LANES = 128
HBM_ARGS = (
    "tokens",
    "w_query",
    "kv_cache",
    "w_key",
    "w_value",
    "head_gain",
    "w_output",
    "attn_norm_gain",
    "w_router",
    "routes",
    "mix_gate",
    "expert_gate",
    "expert_up",
    "dense_gate",
    "dense_up",
    "dense_down",
    "expert_down",
    "ffn_norm_gain",
)


def silu(values):
    return values / (1.0 + jnp.exp(-values))


def layer_kernel(sizes, *refs):
    ep, tp = sizes
    count = len(HBM_ARGS)
    lengths_ref, bias_ref = refs[:2]
    hbm = dict(zip(HBM_ARGS, refs[2 : 2 + count]))
    out_ref, new_kv_ref = refs[2 + count : 4 + count]
    vmem = dict(zip(HBM_ARGS, refs[4 + count : 4 + 2 * count]))
    (
        parts,
        rows,
        mixes,
        stacked,
        hidden,
        outgoing,
        incoming,
        stats,
        load_sem,
        kv_sem,
        part_send,
        part_recv,
        row_send,
        row_recv,
        mix_send,
        mix_recv,
        block_send,
        block_recv,
        stat_send,
        stat_recv,
    ) = refs[4 + 2 * count :]
    e = lax.axis_index("ep")
    t = lax.axis_index("tp")
    seqs, width = vmem["tokens"].shape
    positions, kv_width = vmem["kv_cache"].shape[1:]
    head_dim = kv_width // 2
    experts = vmem["w_router"].shape[1]
    columns = vmem["expert_gate"].shape[1]
    slice_width = width // tp
    devices = ep * tp
    me = e * tp + t

    barrier = pltpu.get_barrier_semaphore()

    def greet(k, carry):
        peer = lax.rem(me + k, devices)
        pl.semaphore_signal(
            barrier,
            inc=1,
            device_id=(peer // tp, lax.rem(peer, tp)),
            device_id_type=pl.DeviceIdType.MESH,
        )
        return carry

    def load(name):
        return pltpu.make_async_copy(hbm[name], vmem[name], load_sem.at[HBM_ARGS.index(name)])

    def load_kv(b):
        return pltpu.make_async_copy(
            hbm["kv_cache"].at[b, 0], vmem["kv_cache"].at[b], kv_sem.at[b]
        )

    for name in HBM_ARGS:
        if name == "kv_cache":
            for b in range(seqs):
                load_kv(b).start()
        else:
            load(name).start()
    lax.fori_loop(1, devices, greet, 0)

    load("tokens").wait()
    load("w_query").wait()
    tokens = vmem["tokens"][...]
    queries = jnp.dot(tokens, vmem["w_query"][...], preferred_element_type=jnp.float32)
    queries = queries.astype(jnp.bfloat16).astype(jnp.float32)
    lane = lax.broadcasted_iota(jnp.int32, (1, kv_width), 1)
    stack = jnp.concatenate([queries, pltpu.roll(queries, head_dim, 1)], axis=0)
    stack = jnp.where(lane < head_dim, stack, 0.0)
    pairs = stack.shape[0]
    row = lax.broadcasted_iota(jnp.int32, (pairs, 1), 0)
    owner = lax.rem(row, seqs)
    scores = jnp.zeros((pairs, positions), jnp.float32)
    for b in range(seqs):
        load_kv(b).wait()
        own = jnp.where(owner == b, stack, 0.0).astype(jnp.bfloat16)
        scores += lax.dot_general(
            own,
            vmem["kv_cache"][b],
            (((1,), (1,)), ((), ())),
            preferred_element_type=jnp.float32,
        )
    limit = jnp.zeros((pairs, 1), jnp.int32)
    for b in range(seqs):
        limit = jnp.where(owner == b, lengths_ref[b], limit)
    bias = jnp.where(row < seqs, bias_ref[0], bias_ref[1])
    z = scores * head_dim ** (-0.5) + bias
    visible = lax.broadcasted_iota(jnp.int32, (pairs, positions), 1) < limit
    tail = jnp.log1p(jnp.exp(-jnp.abs(z)))
    survive = jnp.where(visible, -(jnp.maximum(z, 0.0) + tail), 0.0)
    blocks = positions // LANES
    tall = jnp.concatenate(
        [survive[:, j * LANES : (j + 1) * LANES] for j in range(blocks)], axis=0
    )
    high = tall.astype(jnp.bfloat16)
    rest = tall - high.astype(jnp.float32)
    middle = rest.astype(jnp.bfloat16)
    low = (rest - middle.astype(jnp.float32)).astype(jnp.bfloat16)
    later = (
        lax.broadcasted_iota(jnp.int32, (LANES, LANES), 0)
        > lax.broadcasted_iota(jnp.int32, (LANES, LANES), 1)
    ).astype(jnp.float32).astype(jnp.bfloat16)
    sums = jnp.dot(
        jnp.concatenate([high, middle, low], axis=0), later, preferred_element_type=jnp.float32
    )
    height = blocks * pairs
    sums = sums[:height] + sums[height : 2 * height] + sums[2 * height :]
    totals = jnp.sum(tall, axis=1, keepdims=True)
    running = jnp.zeros((pairs, 1), jnp.float32)
    pieces = [None] * blocks
    for j in reversed(range(blocks)):
        pieces[j] = sums[j * pairs : (j + 1) * pairs] + running
        running = running + totals[j * pairs : (j + 1) * pairs]
    remaining = jnp.concatenate(pieces, axis=1)
    weights = jnp.where(visible, jnp.exp(jnp.minimum(z, 0.0) - tail + remaining), 0.0)
    blended = jnp.zeros((pairs, kv_width), jnp.float32)
    for b in range(seqs):
        own = jnp.where(owner == b, weights, 0.0).astype(jnp.bfloat16)
        blended += jnp.dot(own, vmem["kv_cache"][b], preferred_element_type=jnp.float32)
    blended = jnp.where(lane >= head_dim, blended, 0.0)
    spread = jnp.sum(blended * blended, axis=1, keepdims=True) / head_dim
    blended = blended * lax.rsqrt(spread + 1e-06)
    load("head_gain").wait()
    normed = pltpu.roll(blended[:seqs], head_dim, 1) + blended[seqs:]
    normed = (normed * vmem["head_gain"][...]).astype(jnp.bfloat16)
    load("w_output").wait()
    partial = jnp.dot(normed, vmem["w_output"][...], preferred_element_type=jnp.float32)
    parts[t] = partial.astype(jnp.bfloat16)

    pl.semaphore_wait(barrier, devices - 1)

    def to_tp(buffer, send, recv, peer, slot):
        return pltpu.make_async_remote_copy(
            src_ref=buffer.at[slot],
            dst_ref=buffer.at[slot],
            send_sem=send.at[peer],
            recv_sem=recv.at[slot],
            device_id=(e, peer),
            device_id_type=pl.DeviceIdType.MESH,
        )

    def to_ep(buffer, send, recv, peer, slot):
        return pltpu.make_async_remote_copy(
            src_ref=buffer.at[slot],
            dst_ref=buffer.at[slot],
            send_sem=send.at[peer],
            recv_sem=recv.at[slot],
            device_id=(peer, t),
            device_id_type=pl.DeviceIdType.MESH,
        )

    def tp_peer(k):
        return lax.rem(t + k, tp)

    def ep_peer(k):
        return lax.rem(e + k, ep)

    for k in range(1, tp):
        to_tp(parts, part_send, part_recv, tp_peer(k), t).start()

    load("w_key").wait()
    load("w_value").wait()
    key_new = jnp.dot(tokens, vmem["w_key"][...], preferred_element_type=jnp.float32)
    value_new = jnp.dot(tokens, vmem["w_value"][...], preferred_element_type=jnp.float32)
    new_kv_ref[...] = jnp.concatenate([key_new, value_new], axis=1).astype(jnp.bfloat16)

    load("attn_norm_gain").wait()
    for k in range(1, tp):
        to_tp(parts, part_send, part_recv, tp_peer(k), tp_peer(k)).wait_recv()
    attended = jnp.sum(parts[...].astype(jnp.float32), axis=0)
    settled = layer_norm(
        RESIDUAL_SCALE * tokens.astype(jnp.float32) + attended, vmem["attn_norm_gain"][...]
    ).astype(jnp.bfloat16)
    rows[e] = settled
    for k in range(1, ep):
        to_ep(rows, row_send, row_recv, ep_peer(k), e).start()

    load("w_router").wait()
    load("routes").wait()
    load("mix_gate").wait()
    logits = jnp.dot(settled, vmem["w_router"][...], preferred_element_type=jnp.float32)
    expert_lane = lax.broadcasted_iota(jnp.int32, (seqs, experts), 1)
    routes = vmem["routes"][...]
    first, second = routes[:, :1], routes[:, 1:2]
    first_logit = jnp.sum(jnp.where(expert_lane == first, logits, 0.0), axis=1, keepdims=True)
    second_logit = jnp.sum(jnp.where(expert_lane == second, logits, 0.0), axis=1, keepdims=True)
    settled_wide = settled.astype(jnp.float32)
    mix = jax.nn.sigmoid(
        jnp.sum(settled_wide * vmem["mix_gate"][...].astype(jnp.float32), axis=1, keepdims=True)
    )
    wide_lane = lax.broadcasted_iota(jnp.int32, (seqs, LANES), 1)
    mixes[e] = (
        jnp.where(wide_lane == first, jax.nn.sigmoid(first_logit - second_logit), 0.0)
        + jnp.where(wide_lane == second, jax.nn.sigmoid(second_logit - first_logit), 0.0)
        + jnp.where(wide_lane == experts, mix, 0.0)
    )
    for k in range(1, ep):
        to_ep(mixes, mix_send, mix_recv, ep_peer(k), e).start()

    for name in ("expert_gate", "expert_up", "dense_gate", "dense_up", "dense_down"):
        load(name).wait()
    for k in range(1, ep):
        to_ep(rows, row_send, row_recv, ep_peer(k), ep_peer(k)).wait_recv()
    stacked[...] = jnp.concatenate(
        [rows[i].astype(jnp.float32) for i in range(ep)], axis=0
    ).astype(jnp.bfloat16)

    tile = 256 if columns % 256 == 0 else LANES

    def up_tile(i, carry):
        at = pl.ds(pl.multiple_of(i * tile, tile), tile)
        gate_pre = jnp.dot(
            stacked[...], vmem["expert_gate"][:, at], preferred_element_type=jnp.float32
        )
        up_pre = jnp.dot(
            stacked[...], vmem["expert_up"][:, at], preferred_element_type=jnp.float32
        )
        hidden[:, at] = (silu(gate_pre) * up_pre).astype(jnp.bfloat16)
        return carry

    lax.fori_loop(0, columns // tile, up_tile, 0)
    gate_pre = jnp.dot(
        stacked[...], vmem["dense_gate"][...], preferred_element_type=jnp.float32
    )
    up_pre = jnp.dot(stacked[...], vmem["dense_up"][...], preferred_element_type=jnp.float32)
    dense_hidden = (silu(gate_pre) * up_pre).astype(jnp.bfloat16)
    dense = jnp.dot(dense_hidden, vmem["dense_down"][...], preferred_element_type=jnp.float32)

    for k in range(1, ep):
        to_ep(mixes, mix_send, mix_recv, ep_peer(k), ep_peer(k)).wait_recv()
    table = mixes[...].reshape(ep * seqs, LANES)
    own_expert = me * experts // devices
    all_lane = lax.broadcasted_iota(jnp.int32, (ep * seqs, LANES), 1)
    expert_weight = jnp.sum(jnp.where(all_lane == own_expert, table, 0.0), axis=1, keepdims=True)
    dense_weight = jnp.sum(jnp.where(all_lane == experts, table, 0.0), axis=1, keepdims=True)
    dense = dense * dense_weight

    def block_copy(source, target, send_slot, recv_slot, to_e, to_t):
        return pltpu.make_async_remote_copy(
            src_ref=outgoing.at[source],
            dst_ref=incoming.at[target],
            send_sem=block_send.at[send_slot],
            recv_sem=block_recv.at[recv_slot],
            device_id=(to_e, to_t),
            device_id_type=pl.DeviceIdType.MESH,
        )

    load("expert_down").wait()
    for j in range(tp):
        value = jnp.dot(
            hidden[...],
            vmem["expert_down"][:, j * slice_width : (j + 1) * slice_width],
            preferred_element_type=jnp.float32,
        )
        value = value * expert_weight + jnp.where(t == j, dense, 0.0)
        for i in range(ep):
            outgoing[i * tp + j] = value[i * seqs : (i + 1) * seqs].astype(jnp.bfloat16)

        def send_block(k, carry, j=j):
            to_e = ep_peer(k)
            peer = to_e * tp + j

            @pl.when(peer != me)
            def _():
                block_copy(peer, me, peer, me, to_e, j).start()

            return carry

        lax.fori_loop(0, ep, send_block, 0)
    incoming[me] = outgoing[me]
    load("ffn_norm_gain").wait()

    def wait_block(k, carry):
        peer = lax.rem(me + k, devices)
        block_copy(peer, peer, peer, peer, peer // tp, lax.rem(peer, tp)).wait_recv()
        return carry

    lax.fori_loop(1, devices, wait_block, 0)
    combined = jnp.sum(incoming[...].astype(jnp.float32), axis=0)
    mine = jnp.zeros((seqs, slice_width), jnp.float32)
    for j in range(tp):
        mine = jnp.where(t == j, settled_wide[:, j * slice_width : (j + 1) * slice_width], mine)
    combined = combined + RESIDUAL_SCALE * mine
    row_sum = jnp.sum(combined, axis=1, keepdims=True)
    square = jnp.sum(combined * combined, axis=1, keepdims=True)
    stats[t] = jnp.where(wide_lane == 0, row_sum, jnp.where(wide_lane == 1, square, 0.0))
    for k in range(1, tp):
        to_tp(stats, stat_send, stat_recv, tp_peer(k), t).start()
    for k in range(1, tp):
        to_tp(stats, stat_send, stat_recv, tp_peer(k), tp_peer(k)).wait_recv()
    both = jnp.sum(stats[...], axis=0)
    row_mean = both[:, :1] / width
    row_var = both[:, 1:2] / width - row_mean * row_mean
    out_ref[...] = (
        (combined - row_mean) * lax.rsqrt(row_var + 1e-05) * vmem["ffn_norm_gain"][...]
    ).astype(jnp.bfloat16)

    for k in range(1, tp):
        to_tp(parts, part_send, part_recv, tp_peer(k), t).wait_send()
        to_tp(stats, stat_send, stat_recv, tp_peer(k), t).wait_send()
    for k in range(1, ep):
        to_ep(rows, row_send, row_recv, ep_peer(k), e).wait_send()
        to_ep(mixes, mix_send, mix_recv, ep_peer(k), e).wait_send()

    def drain(k, carry):
        peer = lax.rem(me + k, devices)
        block_copy(peer, me, peer, me, peer // tp, lax.rem(peer, tp)).wait_send()
        return carry

    lax.fori_loop(1, devices, drain, 0)


NAMES = (
    "tokens",
    "kv_cache",
    "lengths",
    "w_query",
    "w_key",
    "w_value",
    "break_bias",
    "head_gain",
    "w_output",
    "attn_norm_gain",
    "w_router",
    "routes",
    "expert_gate",
    "expert_up",
    "expert_down",
    "dense_gate",
    "dense_up",
    "dense_down",
    "mix_gate",
    "ffn_norm_gain",
)


def fused_fits(args, ep, tp):
    seqs, width = args["tokens"].shape
    _, key_heads, positions, kv_width = args["kv_cache"].shape
    experts = args["w_router"].shape[1]
    return (
        seqs == 8
        and key_heads == 1
        and kv_width == LANES
        and args["w_query"].shape[1] == LANES
        and positions % LANES == 0
        and experts < LANES
        and args["routes"].shape[1] == 2
        and (ep * tp) % experts == 0
        and args["expert_gate"].shape[1] % LANES == 0
        and (width // tp) % LANES == 0
    )


def fused(args, ep, tp):
    for name in ("head_gain", "attn_norm_gain", "mix_gate", "ffn_norm_gain"):
        args[name] = args[name].reshape(1, -1)
    operands = [args[name] for name in HBM_ARGS]
    seqs, width = args["tokens"].shape
    slice_width = width // tp
    devices = ep * tp
    scratch = []
    for name, operand in zip(HBM_ARGS, operands):
        shape = operand.shape
        if name == "kv_cache":
            shape = (shape[0],) + shape[2:]
        scratch.append(pltpu.VMEM(shape, operand.dtype))
    dma = pltpu.SemaphoreType.DMA
    scratch += [
        pltpu.VMEM((tp, seqs, width), jnp.bfloat16),
        pltpu.VMEM((ep, seqs, width), jnp.bfloat16),
        pltpu.VMEM((ep, seqs, LANES), jnp.float32),
        pltpu.VMEM((ep * seqs, width), jnp.bfloat16),
        pltpu.VMEM((ep * seqs, args["expert_gate"].shape[1]), jnp.bfloat16),
        pltpu.VMEM((devices, seqs, slice_width), jnp.bfloat16),
        pltpu.VMEM((devices, seqs, slice_width), jnp.bfloat16),
        pltpu.VMEM((tp, seqs, LANES), jnp.float32),
        dma((len(HBM_ARGS),)),
        dma((seqs,)),
        dma((tp,)),
        dma((tp,)),
        dma((ep,)),
        dma((ep,)),
        dma((ep,)),
        dma((ep,)),
        dma((devices,)),
        dma((devices,)),
        dma((tp,)),
        dma((tp,)),
    ]
    smem = pl.BlockSpec(memory_space=pltpu.SMEM)
    result, new_kv = pl.pallas_call(
        functools.partial(layer_kernel, (ep, tp)),
        out_shape=(
            jax.ShapeDtypeStruct((seqs, slice_width), jnp.bfloat16),
            jax.ShapeDtypeStruct((seqs, LANES), jnp.bfloat16),
        ),
        in_specs=[smem, smem] + [pl.BlockSpec(memory_space=pl.ANY)] * len(HBM_ARGS),
        out_specs=(
            pl.BlockSpec(memory_space=pltpu.VMEM),
            pl.BlockSpec(memory_space=pltpu.VMEM),
        ),
        scratch_shapes=scratch,
        compiler_params=pltpu.CompilerParams(
            collective_id=0, has_side_effects=True, vmem_limit_bytes=60 * 1024 * 1024
        ),
    )(args["lengths"], args["break_bias"], *operands)
    return result, new_kv.reshape(seqs, 1, LANES)


def layer(ep, tp, *arrays):
    args = dict(zip(NAMES, arrays))
    if fused_fits(args, ep, tp):
        return fused(args, ep, tp)
    return body(*arrays)


def solution(mesh):
    in_specs = (
        P("ep", None),
        P("ep", "tp", None, None),
        P("ep"),
        P(None, "tp"),
        P(None, "tp"),
        P(None, "tp"),
        P("tp"),
        P("tp"),
        P("tp", None),
        P(),
        P(),
        P("ep", None),
        P(None, ("ep", "tp")),
        P(None, ("ep", "tp")),
        P(("ep", "tp"), None),
        P(None, "ep"),
        P(None, "ep"),
        P("ep", "tp"),
        P(),
        P("tp"),
    )
    out_specs = (P("ep", "tp"), P("ep", "tp", None))
    step = functools.partial(layer, mesh.shape["ep"], mesh.shape["tp"])
    return jax.shard_map(step, mesh=mesh, in_specs=in_specs, out_specs=out_specs, check_vma=False)
```

```python
import functools

import jax
import jax.numpy as jnp
from jax import lax
from jax.experimental import pallas as pl
from jax.experimental.pallas import tpu as pltpu
from jax.sharding import PartitionSpec as P

FE = 3584
CAP = 2


RESIDUAL_SCALE = 8.0**0.25
PRECISE = lax.Precision.HIGHEST


def layer_norm(values, gain):
    centre = jnp.mean(values, axis=-1, keepdims=True)
    centred = values - centre
    spread = jnp.mean(centred * centred, axis=-1, keepdims=True)
    return centred * lax.rsqrt(spread + 1e-05) * gain


def stick_weights(scores, visible):
    survive = jnp.where(visible, jax.nn.log_sigmoid(-scores), 0.0)
    remaining = lax.cumsum(survive, axis=3, reverse=True) - survive
    return jnp.where(visible, jnp.exp(jax.nn.log_sigmoid(scores) + remaining), 0.0)


def body(
    tokens,
    kv_cache,
    lengths,
    w_query,
    w_key,
    w_value,
    break_bias,
    head_gain,
    w_output,
    attn_norm_gain,
    w_router,
    routes,
    expert_gate,
    expert_up,
    expert_down,
    dense_gate,
    dense_up,
    dense_down,
    mix_gate,
    ffn_norm_gain,
):
    seq_count = tokens.shape[0]
    model_width = tokens.shape[1]
    key_heads = kv_cache.shape[1]
    positions = kv_cache.shape[2]
    head_dim = kv_cache.shape[3] // 2
    local_heads = w_query.shape[1] // head_dim
    group_size = local_heads // key_heads
    queries = jnp.dot(tokens, w_query, preferred_element_type=jnp.float32).astype(jnp.bfloat16)
    queries = queries.reshape(seq_count, key_heads, group_size, head_dim)
    key_new = jnp.dot(tokens, w_key, preferred_element_type=jnp.float32).astype(jnp.bfloat16)
    value_new = jnp.dot(tokens, w_value, preferred_element_type=jnp.float32).astype(jnp.bfloat16)
    new_kv = jnp.concatenate(
        [
            key_new.reshape(seq_count, key_heads, head_dim),
            value_new.reshape(seq_count, key_heads, head_dim),
        ],
        axis=2,
    )
    cached_keys = kv_cache[..., :head_dim]
    cached_values = kv_cache[..., head_dim:]
    scores = jnp.einsum(
        "bgqd,bgld->bgql", queries, cached_keys, preferred_element_type=jnp.float32
    ) * head_dim ** (-0.5)
    scores = scores + break_bias.reshape(1, key_heads, group_size, 1)
    visible = lax.broadcasted_iota(jnp.int32, (seq_count, 1, 1, positions), 3) < lengths.reshape(
        seq_count, 1, 1, 1
    )
    weights = stick_weights(scores, visible).astype(jnp.bfloat16)
    blended = jnp.einsum(
        "bgql,bgld->bgqd", weights, cached_values, preferred_element_type=jnp.float32
    )
    rescale = lax.rsqrt(jnp.mean(blended * blended, axis=3, keepdims=True) + 1e-06)
    normed = ((blended * rescale).reshape(seq_count, local_heads * head_dim) * head_gain).astype(
        jnp.bfloat16
    )
    partial_out = jnp.dot(normed, w_output, preferred_element_type=jnp.float32)
    attended = lax.psum(partial_out.astype(jnp.bfloat16), "tp").astype(jnp.float32)
    settled = layer_norm(
        RESIDUAL_SCALE * tokens.astype(jnp.float32) + attended, attn_norm_gain
    ).astype(jnp.bfloat16)
    experts = w_router.shape[1]
    top_count = routes.shape[1]
    logits = jnp.dot(settled, w_router, preferred_element_type=jnp.float32)
    chosen = routes[:, :, None] == lax.broadcasted_iota(
        jnp.int32, (seq_count, top_count, experts), 2
    )
    picked = jnp.sum(jnp.where(chosen, logits[:, None, :], 0.0), axis=2)
    route_weight = jax.nn.sigmoid(picked - picked[:, ::-1])
    assigned = chosen.reshape(seq_count * top_count, experts).astype(jnp.int32)
    before = jnp.cumsum(assigned, axis=0) - assigned
    slot_index = jnp.sum(before * assigned, axis=1)
    slot_hits = (
        slot_index[:, None] == lax.broadcasted_iota(jnp.int32, (seq_count * top_count, CAP), 1)
    ).astype(jnp.int32)
    placement = (assigned[:, :, None] * slot_hits[:, None, :]).reshape(
        seq_count, top_count, experts * CAP
    )
    selector = jnp.sum(placement, axis=1).astype(jnp.bfloat16)
    weighted = jnp.sum(placement.astype(jnp.float32) * route_weight[:, :, None], axis=1)
    buffer = lax.dot_general(
        selector, settled, (((0,), (0,)), ((), ())), preferred_element_type=jnp.float32
    )
    buffer = buffer.astype(jnp.bfloat16).reshape(experts, CAP, model_width)
    hosts = lax.axis_size("ep")
    tp_size = lax.axis_size("tp")
    if experts >= hosts:
        per_host = experts // hosts
        outgoing = buffer.reshape(hosts, per_host, CAP, model_width)
    else:
        per_host = 1
        outgoing = jnp.repeat(buffer, hosts // experts, axis=0).reshape(hosts, 1, CAP, model_width)
    columns = expert_gate.shape[1]
    block_index = lax.axis_index(("ep", "tp"))
    own_expert = block_index * columns // FE
    local_slot = own_expert - lax.axis_index("ep") * experts // hosts
    slice_width = model_width // tp_size
    arrived = lax.all_to_all(outgoing, "ep", split_axis=0, concat_axis=0, tiled=True)
    slot_count = arrived.shape[2]
    received = lax.dynamic_index_in_dim(arrived, local_slot, 1, keepdims=False)
    received = received.reshape(hosts * slot_count, model_width)
    gate_pre = jnp.dot(received, expert_gate, preferred_element_type=jnp.float32)
    up_pre = jnp.dot(received, expert_up, preferred_element_type=jnp.float32)
    hidden = (jax.nn.silu(gate_pre) * up_pre).astype(jnp.bfloat16)
    partial_value = jnp.dot(hidden, expert_down, preferred_element_type=jnp.float32)
    partial_value = partial_value.reshape(hosts, 1, slot_count, model_width)
    slot_mask = (lax.broadcasted_iota(jnp.int32, (1, per_host, 1, 1), 1) == local_slot).astype(
        jnp.float32
    )
    summed = lax.psum_scatter(
        (partial_value * slot_mask).astype(jnp.bfloat16), "tp", scatter_dimension=3, tiled=True
    ).astype(jnp.float32)
    returned = lax.all_to_all(
        summed.astype(jnp.bfloat16), "ep", split_axis=0, concat_axis=0, tiled=True
    ).astype(summed.dtype)
    host_ids = lax.broadcasted_iota(jnp.int32, (hosts * per_host,), 0)
    host_expert = host_ids // per_host * experts // hosts + host_ids % per_host
    ownership = (
        host_expert[None, :] == lax.broadcasted_iota(jnp.int32, (experts, hosts * per_host), 0)
    ).astype(jnp.float32)
    gathered = jnp.dot(
        ownership, returned.reshape(hosts * per_host, CAP * slice_width), precision=PRECISE
    )
    gathered = gathered.reshape(experts * CAP, slice_width)
    routed = jnp.dot(weighted, gathered, precision=PRECISE)
    column_rank = lax.axis_index("tp")
    own_settled = lax.dynamic_slice_in_dim(settled, column_rank * slice_width, slice_width, 1)
    shard_rows = lax.all_gather(settled, "ep", axis=0, tiled=True)
    gate_pre = jnp.dot(shard_rows, dense_gate, preferred_element_type=jnp.float32)
    up_pre = jnp.dot(shard_rows, dense_up, preferred_element_type=jnp.float32)
    dense_hidden = (jax.nn.silu(gate_pre) * up_pre).astype(jnp.bfloat16)
    own_hidden = lax.all_to_all(dense_hidden, "ep", split_axis=0, concat_axis=1, tiled=True)
    dense_out = jnp.dot(
        own_hidden,
        lax.all_gather(dense_down, "ep", axis=0, tiled=True),
        preferred_element_type=jnp.float32,
    )
    mix_weight = jax.nn.sigmoid(jnp.dot(settled, mix_gate, preferred_element_type=jnp.float32))
    combined = (
        RESIDUAL_SCALE * own_settled.astype(jnp.float32) + routed + mix_weight[:, None] * dense_out
    )
    row_sums, squares = lax.psum(
        (jnp.sum(combined, axis=1), jnp.sum(combined * combined, axis=1)), "tp"
    )
    row_mean = row_sums / model_width
    row_var = squares / model_width - row_mean * row_mean
    result = (
        (combined - row_mean[:, None]) * lax.rsqrt(row_var[:, None] + 1e-05) * ffn_norm_gain
    ).astype(jnp.bfloat16)
    return (result, new_kv)


LANES = 128
HBM_ARGS = (
    "tokens",
    "w_query",
    "kv_cache",
    "w_key",
    "w_value",
    "head_gain",
    "w_output",
    "attn_norm_gain",
    "w_router",
    "mix_gate",
    "expert_gate",
    "expert_up",
    "dense_gate",
    "dense_up",
    "dense_down",
    "expert_down",
    "ffn_norm_gain",
)


def silu(values):
    return values / (1.0 + jnp.exp(-values))


def dot_rows(left, right):
    return lax.dot_general(
        left, right, (((1,), (1,)), ((), ())), preferred_element_type=jnp.float32
    )


def layer_kernel(sizes, *refs):
    ep, tp = sizes
    count = len(HBM_ARGS)
    lengths_ref, bias_ref, routes_ref = refs[:3]
    hbm = dict(zip(HBM_ARGS, refs[3 : 3 + count]))
    out_ref, new_kv_ref = refs[3 + count : 5 + count]
    vmem = dict(zip(HBM_ARGS, refs[5 + count : 5 + 2 * count]))
    (
        parts,
        rows,
        mixes,
        stacked,
        hidden,
        outgoing,
        incoming,
        stats,
        load_sem,
        kv_sem,
        part_send,
        part_recv,
        row_send,
        row_recv,
        mix_send,
        mix_recv,
        block_send,
        block_recv,
        stat_send,
        stat_recv,
    ) = refs[5 + 2 * count :]
    e = lax.axis_index("ep")
    t = lax.axis_index("tp")
    seqs, width = vmem["tokens"].shape
    positions, kv_width = vmem["kv_cache"].shape[1:]
    head_dim = kv_width // 2
    experts = vmem["w_router"].shape[0]
    columns = vmem["expert_gate"].shape[1]
    slice_width = width // tp
    devices = ep * tp
    me = e * tp + t

    barrier = pltpu.get_barrier_semaphore()

    def greet(k, carry):
        peer = lax.rem(me + k, devices)
        pl.semaphore_signal(
            barrier,
            inc=1,
            device_id=(peer // tp, lax.rem(peer, tp)),
            device_id_type=pl.DeviceIdType.MESH,
        )
        return carry

    def load(name):
        return pltpu.make_async_copy(hbm[name], vmem[name], load_sem.at[HBM_ARGS.index(name)])

    def load_kv(b):
        return pltpu.make_async_copy(
            hbm["kv_cache"].at[b, 0], vmem["kv_cache"].at[b], kv_sem.at[b]
        )

    for name in HBM_ARGS:
        if name == "kv_cache":
            for b in range(seqs):
                load_kv(b).start()
        else:
            load(name).start()
    lax.fori_loop(1, devices, greet, 0)

    load("tokens").wait()
    load("w_query").wait()
    tokens = vmem["tokens"][...]
    queries = jnp.dot(tokens, vmem["w_query"][...], preferred_element_type=jnp.float32)
    queries = queries.astype(jnp.bfloat16).astype(jnp.float32)
    lane = lax.broadcasted_iota(jnp.int32, (1, kv_width), 1)
    stack = jnp.concatenate([queries, pltpu.roll(queries, head_dim, 1)], axis=0)
    stack = jnp.where(lane < head_dim, stack, 0.0)
    pairs = stack.shape[0]
    row = lax.broadcasted_iota(jnp.int32, (pairs, 1), 0)
    owner = lax.rem(row, seqs)
    scores = jnp.zeros((pairs, positions), jnp.float32)
    for b in range(seqs):
        load_kv(b).wait()
        own = jnp.where(owner == b, stack, 0.0).astype(jnp.bfloat16)
        scores += dot_rows(own, vmem["kv_cache"][b])
    limit = jnp.zeros((pairs, 1), jnp.int32)
    for b in range(seqs):
        limit = jnp.where(owner == b, lengths_ref[b], limit)
    bias = jnp.where(row < seqs, bias_ref[0], bias_ref[1])
    z = scores * head_dim ** (-0.5) + bias
    visible = lax.broadcasted_iota(jnp.int32, (pairs, positions), 1) < limit
    tail = jnp.log1p(jnp.exp(-jnp.abs(z)))
    survive = jnp.where(visible, -(jnp.maximum(z, 0.0) + tail), 0.0)
    blocks = positions // LANES
    tall = jnp.concatenate(
        [survive[:, j * LANES : (j + 1) * LANES] for j in range(blocks)], axis=0
    )
    high = tall.astype(jnp.bfloat16)
    rest = tall - high.astype(jnp.float32)
    middle = rest.astype(jnp.bfloat16)
    low = (rest - middle.astype(jnp.float32)).astype(jnp.bfloat16)
    later = (
        lax.broadcasted_iota(jnp.int32, (LANES, LANES), 0)
        > lax.broadcasted_iota(jnp.int32, (LANES, LANES), 1)
    ).astype(jnp.float32).astype(jnp.bfloat16)
    sums = jnp.dot(
        jnp.concatenate([high, middle, low], axis=0), later, preferred_element_type=jnp.float32
    )
    height = blocks * pairs
    sums = sums[:height] + sums[height : 2 * height] + sums[2 * height :]
    totals = jnp.sum(tall, axis=1, keepdims=True)
    running = jnp.zeros((pairs, 1), jnp.float32)
    pieces = [None] * blocks
    for j in reversed(range(blocks)):
        pieces[j] = sums[j * pairs : (j + 1) * pairs] + running
        running = running + totals[j * pairs : (j + 1) * pairs]
    remaining = jnp.concatenate(pieces, axis=1)
    weights = jnp.where(visible, jnp.exp(jnp.minimum(z, 0.0) - tail + remaining), 0.0)
    blended = jnp.zeros((pairs, kv_width), jnp.float32)
    for b in range(seqs):
        own = jnp.where(owner == b, weights, 0.0).astype(jnp.bfloat16)
        blended += jnp.dot(own, vmem["kv_cache"][b], preferred_element_type=jnp.float32)
    blended = jnp.where(lane >= head_dim, blended, 0.0)
    spread = jnp.sum(blended * blended, axis=1, keepdims=True) / head_dim
    blended = blended * lax.rsqrt(spread + 1e-06)
    load("head_gain").wait()
    normed = pltpu.roll(blended[:seqs], head_dim, 1) + blended[seqs:]
    normed = (normed * vmem["head_gain"][...]).astype(jnp.bfloat16)
    load("w_output").wait()
    partial = jnp.dot(normed, vmem["w_output"][...], preferred_element_type=jnp.float32)
    parts[t] = partial.astype(jnp.bfloat16)

    pl.semaphore_wait(barrier, devices - 1)

    def to_tp(buffer, send, recv, peer, slot):
        return pltpu.make_async_remote_copy(
            src_ref=buffer.at[slot],
            dst_ref=buffer.at[slot],
            send_sem=send.at[peer],
            recv_sem=recv.at[slot],
            device_id=(e, peer),
            device_id_type=pl.DeviceIdType.MESH,
        )

    def to_ep(buffer, send, recv, peer, slot):
        return pltpu.make_async_remote_copy(
            src_ref=buffer.at[slot],
            dst_ref=buffer.at[slot],
            send_sem=send.at[peer],
            recv_sem=recv.at[slot],
            device_id=(peer, t),
            device_id_type=pl.DeviceIdType.MESH,
        )

    def tp_peer(k):
        return lax.rem(t + k, tp)

    def ep_peer(k):
        return lax.rem(e + k, ep)

    for k in range(1, tp):
        to_tp(parts, part_send, part_recv, tp_peer(k), t).start()

    load("w_key").wait()
    load("w_value").wait()
    key_new = dot_rows(tokens, vmem["w_key"][...])
    value_new = dot_rows(tokens, vmem["w_value"][...])
    new_kv_ref[...] = jnp.concatenate([key_new, value_new], axis=1).astype(jnp.bfloat16)

    load("attn_norm_gain").wait()
    for k in range(1, tp):
        to_tp(parts, part_send, part_recv, tp_peer(k), tp_peer(k)).wait_recv()
    attended = jnp.sum(parts[...].astype(jnp.float32), axis=0)
    settled = layer_norm(
        RESIDUAL_SCALE * tokens.astype(jnp.float32) + attended, vmem["attn_norm_gain"][...]
    ).astype(jnp.bfloat16)
    rows[e] = settled
    for k in range(1, ep):
        to_ep(rows, row_send, row_recv, ep_peer(k), e).start()

    load("w_router").wait()
    load("mix_gate").wait()
    logits = dot_rows(settled, vmem["w_router"][...])
    expert_lane = lax.broadcasted_iota(jnp.int32, (seqs, experts), 1)
    seq_row = lax.broadcasted_iota(jnp.int32, (seqs, 1), 0)
    first = jnp.zeros((seqs, 1), jnp.int32)
    second = jnp.zeros((seqs, 1), jnp.int32)
    for b in range(seqs):
        first = jnp.where(seq_row == b, routes_ref[0, b], first)
        second = jnp.where(seq_row == b, routes_ref[1, b], second)
    first_logit = jnp.sum(jnp.where(expert_lane == first, logits, 0.0), axis=1, keepdims=True)
    second_logit = jnp.sum(jnp.where(expert_lane == second, logits, 0.0), axis=1, keepdims=True)
    settled_wide = settled.astype(jnp.float32)
    mix_gate = vmem["mix_gate"][...].astype(jnp.float32)
    products = jnp.zeros((seqs, LANES), jnp.float32)
    for j in range(width // LANES):
        products += settled_wide[:, j * LANES : (j + 1) * LANES] * mix_gate[j : j + 1]
    mix = jax.nn.sigmoid(jnp.sum(products, axis=1, keepdims=True))
    wide_lane = lax.broadcasted_iota(jnp.int32, (seqs, LANES), 1)
    mixes[e] = (
        jnp.where(wide_lane == first, jax.nn.sigmoid(first_logit - second_logit), 0.0)
        + jnp.where(wide_lane == second, jax.nn.sigmoid(second_logit - first_logit), 0.0)
        + jnp.where(wide_lane == experts, mix, 0.0)
    )
    for k in range(1, ep):
        to_ep(mixes, mix_send, mix_recv, ep_peer(k), e).start()

    for name in ("expert_gate", "expert_up", "dense_gate", "dense_up", "dense_down"):
        load(name).wait()
    for k in range(1, ep):
        to_ep(rows, row_send, row_recv, ep_peer(k), ep_peer(k)).wait_recv()
    stacked[...] = jnp.concatenate(
        [rows[i].astype(jnp.float32) for i in range(ep)], axis=0
    ).astype(jnp.bfloat16)

    tile = 256 if columns % 256 == 0 else LANES

    def up_tile(i, carry):
        at = pl.ds(pl.multiple_of(i * tile, tile), tile)
        gate_pre = jnp.dot(
            stacked[...], vmem["expert_gate"][:, at], preferred_element_type=jnp.float32
        )
        up_pre = jnp.dot(
            stacked[...], vmem["expert_up"][:, at], preferred_element_type=jnp.float32
        )
        hidden[:, at] = (silu(gate_pre) * up_pre).astype(jnp.bfloat16)
        return carry

    lax.fori_loop(0, columns // tile, up_tile, 0)
    gate_pre = dot_rows(stacked[...], vmem["dense_gate"][...])
    up_pre = dot_rows(stacked[...], vmem["dense_up"][...])
    dense_hidden = (silu(gate_pre) * up_pre).astype(jnp.bfloat16)
    dense = jnp.dot(dense_hidden, vmem["dense_down"][...], preferred_element_type=jnp.float32)

    for k in range(1, ep):
        to_ep(mixes, mix_send, mix_recv, ep_peer(k), ep_peer(k)).wait_recv()
    table = mixes[...].reshape(ep * seqs, LANES)
    own_expert = me * experts // devices
    all_lane = lax.broadcasted_iota(jnp.int32, (ep * seqs, LANES), 1)
    expert_weight = jnp.sum(jnp.where(all_lane == own_expert, table, 0.0), axis=1, keepdims=True)
    dense_weight = jnp.sum(jnp.where(all_lane == experts, table, 0.0), axis=1, keepdims=True)
    dense = dense * dense_weight

    def block_copy(source, target, send_slot, recv_slot, to_e, to_t):
        return pltpu.make_async_remote_copy(
            src_ref=outgoing.at[source],
            dst_ref=incoming.at[target],
            send_sem=block_send.at[send_slot],
            recv_sem=block_recv.at[recv_slot],
            device_id=(to_e, to_t),
            device_id_type=pl.DeviceIdType.MESH,
        )

    load("expert_down").wait()
    for j in range(tp):
        value = jnp.dot(
            hidden[...],
            vmem["expert_down"][:, j * slice_width : (j + 1) * slice_width],
            preferred_element_type=jnp.float32,
        )
        value = value * expert_weight + jnp.where(t == j, dense, 0.0)
        for i in range(ep):
            outgoing[i * tp + j] = value[i * seqs : (i + 1) * seqs].astype(jnp.bfloat16)

        def send_block(k, carry, j=j):
            to_e = ep_peer(k)
            peer = to_e * tp + j

            @pl.when(peer != me)
            def _():
                block_copy(peer, me, peer, me, to_e, j).start()

            return carry

        lax.fori_loop(0, ep, send_block, 0)
    incoming[me] = outgoing[me]
    load("ffn_norm_gain").wait()

    def wait_block(k, carry):
        peer = lax.rem(me + k, devices)
        block_copy(peer, peer, peer, peer, peer // tp, lax.rem(peer, tp)).wait_recv()
        return carry

    lax.fori_loop(1, devices, wait_block, 0)
    combined = jnp.sum(incoming[...].astype(jnp.float32), axis=0)
    mine = jnp.zeros((seqs, slice_width), jnp.float32)
    for j in range(tp):
        mine = jnp.where(t == j, settled_wide[:, j * slice_width : (j + 1) * slice_width], mine)
    combined = combined + RESIDUAL_SCALE * mine
    row_sum = jnp.sum(combined, axis=1, keepdims=True)
    square = jnp.sum(combined * combined, axis=1, keepdims=True)
    stats[t] = jnp.where(wide_lane == 0, row_sum, jnp.where(wide_lane == 1, square, 0.0))
    for k in range(1, tp):
        to_tp(stats, stat_send, stat_recv, tp_peer(k), t).start()
    for k in range(1, tp):
        to_tp(stats, stat_send, stat_recv, tp_peer(k), tp_peer(k)).wait_recv()
    both = jnp.sum(stats[...], axis=0)
    row_mean = both[:, :1] / width
    row_var = both[:, 1:2] / width - row_mean * row_mean
    out_ref[...] = (
        (combined - row_mean) * lax.rsqrt(row_var + 1e-05) * vmem["ffn_norm_gain"][...]
    ).astype(jnp.bfloat16)

    for k in range(1, tp):
        to_tp(parts, part_send, part_recv, tp_peer(k), t).wait_send()
        to_tp(stats, stat_send, stat_recv, tp_peer(k), t).wait_send()
    for k in range(1, ep):
        to_ep(rows, row_send, row_recv, ep_peer(k), e).wait_send()
        to_ep(mixes, mix_send, mix_recv, ep_peer(k), e).wait_send()

    def drain(k, carry):
        peer = lax.rem(me + k, devices)
        block_copy(peer, me, peer, me, peer // tp, lax.rem(peer, tp)).wait_send()
        return carry

    lax.fori_loop(1, devices, drain, 0)


def finish_kernel(result_ref, new_kv_ref, result_out, new_kv_out):
    result_out[...] = result_ref[...]
    new_kv_out[...] = new_kv_ref[...]


NAMES = (
    "tokens",
    "kv_cache",
    "lengths",
    "w_query",
    "w_key",
    "w_value",
    "break_bias",
    "head_gain",
    "w_output",
    "attn_norm_gain",
    "w_router",
    "routes",
    "expert_gate",
    "expert_up",
    "expert_down",
    "dense_gate",
    "dense_up",
    "dense_down",
    "mix_gate",
    "ffn_norm_gain",
)


def fused_fits(args, ep, tp):
    seqs, width = args["tokens"].shape
    _, key_heads, positions, kv_width = args["kv_cache"].shape
    experts = args["w_router"].shape[1]
    return (
        seqs == 8
        and key_heads == 1
        and kv_width == LANES
        and args["w_query"].shape[1] == LANES
        and positions % LANES == 0
        and experts < LANES
        and args["routes"].shape[1] == 2
        and (ep * tp) % experts == 0
        and args["expert_gate"].shape[1] % LANES == 0
        and (width // tp) % LANES == 0
    )


def fused(args, ep, tp):
    for name in ("head_gain", "attn_norm_gain", "ffn_norm_gain"):
        args[name] = args[name].reshape(1, -1)
    args["mix_gate"] = args["mix_gate"].reshape(-1, LANES)
    for name in ("w_key", "w_value", "w_router", "routes", "dense_gate", "dense_up"):
        args[name] = args[name].T
    operands = [args[name] for name in HBM_ARGS]
    seqs, width = args["tokens"].shape
    slice_width = width // tp
    devices = ep * tp
    scratch = []
    for name, operand in zip(HBM_ARGS, operands):
        shape = operand.shape
        if name == "kv_cache":
            shape = (shape[0],) + shape[2:]
        scratch.append(pltpu.VMEM(shape, operand.dtype))
    dma = pltpu.SemaphoreType.DMA
    scratch += [
        pltpu.VMEM((tp, seqs, width), jnp.bfloat16),
        pltpu.VMEM((ep, seqs, width), jnp.bfloat16),
        pltpu.VMEM((ep, seqs, LANES), jnp.float32),
        pltpu.VMEM((ep * seqs, width), jnp.bfloat16),
        pltpu.VMEM((ep * seqs, args["expert_gate"].shape[1]), jnp.bfloat16),
        pltpu.VMEM((devices, seqs, slice_width), jnp.bfloat16),
        pltpu.VMEM((devices, seqs, slice_width), jnp.bfloat16),
        pltpu.VMEM((tp, seqs, LANES), jnp.float32),
        dma((len(HBM_ARGS),)),
        dma((seqs,)),
        dma((tp,)),
        dma((tp,)),
        dma((ep,)),
        dma((ep,)),
        dma((ep,)),
        dma((ep,)),
        dma((devices,)),
        dma((devices,)),
        dma((tp,)),
        dma((tp,)),
    ]
    smem = pl.BlockSpec(memory_space=pltpu.SMEM)
    result, new_kv = pl.pallas_call(
        functools.partial(layer_kernel, (ep, tp)),
        out_shape=(
            jax.ShapeDtypeStruct((seqs, slice_width), jnp.bfloat16),
            jax.ShapeDtypeStruct((seqs, LANES), jnp.bfloat16),
        ),
        in_specs=[smem, smem, smem] + [pl.BlockSpec(memory_space=pl.ANY)] * len(HBM_ARGS),
        out_specs=(
            pl.BlockSpec(memory_space=pltpu.VMEM),
            pl.BlockSpec(memory_space=pltpu.VMEM),
        ),
        scratch_shapes=scratch,
        compiler_params=pltpu.CompilerParams(
            collective_id=0, has_side_effects=True, vmem_limit_bytes=60 * 1024 * 1024
        ),
    )(args["lengths"], args["break_bias"], args["routes"], *operands)
    result, new_kv = pl.pallas_call(
        finish_kernel,
        out_shape=(
            jax.ShapeDtypeStruct(result.shape, result.dtype),
            jax.ShapeDtypeStruct(new_kv.shape, new_kv.dtype),
        ),
    )(result, new_kv)
    return result, new_kv.reshape(seqs, 1, LANES)


def layer(ep, tp, *arrays):
    args = dict(zip(NAMES, arrays))
    if fused_fits(args, ep, tp):
        return fused(args, ep, tp)
    return body(*arrays)


def solution(mesh):
    in_specs = (
        P("ep", None),
        P("ep", "tp", None, None),
        P("ep"),
        P(None, "tp"),
        P(None, "tp"),
        P(None, "tp"),
        P("tp"),
        P("tp"),
        P("tp", None),
        P(),
        P(),
        P("ep", None),
        P(None, ("ep", "tp")),
        P(None, ("ep", "tp")),
        P(("ep", "tp"), None),
        P(None, "ep"),
        P(None, "ep"),
        P("ep", "tp"),
        P(),
        P("tp"),
    )
    out_specs = (P("ep", "tp"), P("ep", "tp", None))
    step = functools.partial(layer, mesh.shape["ep"], mesh.shape["tp"])
    return jax.shard_map(step, mesh=mesh, in_specs=in_specs, out_specs=out_specs, check_vma=False)
```

```python
import functools

import jax
import jax.numpy as jnp
from jax import lax
from jax.experimental import pallas as pl
from jax.experimental.pallas import tpu as pltpu
from jax.sharding import PartitionSpec as P

FE = 3584
CAP = 2


RESIDUAL_SCALE = 8.0**0.25
PRECISE = lax.Precision.HIGHEST


def layer_norm(values, gain):
    centre = jnp.mean(values, axis=-1, keepdims=True)
    centred = values - centre
    spread = jnp.mean(centred * centred, axis=-1, keepdims=True)
    return centred * lax.rsqrt(spread + 1e-05) * gain


def stick_weights(scores, visible):
    survive = jnp.where(visible, jax.nn.log_sigmoid(-scores), 0.0)
    remaining = lax.cumsum(survive, axis=3, reverse=True) - survive
    return jnp.where(visible, jnp.exp(jax.nn.log_sigmoid(scores) + remaining), 0.0)


def body(
    tokens,
    kv_cache,
    lengths,
    w_query,
    w_key,
    w_value,
    break_bias,
    head_gain,
    w_output,
    attn_norm_gain,
    w_router,
    routes,
    expert_gate,
    expert_up,
    expert_down,
    dense_gate,
    dense_up,
    dense_down,
    mix_gate,
    ffn_norm_gain,
):
    seq_count = tokens.shape[0]
    model_width = tokens.shape[1]
    key_heads = kv_cache.shape[1]
    positions = kv_cache.shape[2]
    head_dim = kv_cache.shape[3] // 2
    local_heads = w_query.shape[1] // head_dim
    group_size = local_heads // key_heads
    queries = jnp.dot(tokens, w_query, preferred_element_type=jnp.float32).astype(jnp.bfloat16)
    queries = queries.reshape(seq_count, key_heads, group_size, head_dim)
    key_new = jnp.dot(tokens, w_key, preferred_element_type=jnp.float32).astype(jnp.bfloat16)
    value_new = jnp.dot(tokens, w_value, preferred_element_type=jnp.float32).astype(jnp.bfloat16)
    new_kv = jnp.concatenate(
        [
            key_new.reshape(seq_count, key_heads, head_dim),
            value_new.reshape(seq_count, key_heads, head_dim),
        ],
        axis=2,
    )
    cached_keys = kv_cache[..., :head_dim]
    cached_values = kv_cache[..., head_dim:]
    scores = jnp.einsum(
        "bgqd,bgld->bgql", queries, cached_keys, preferred_element_type=jnp.float32
    ) * head_dim ** (-0.5)
    scores = scores + break_bias.reshape(1, key_heads, group_size, 1)
    visible = lax.broadcasted_iota(jnp.int32, (seq_count, 1, 1, positions), 3) < lengths.reshape(
        seq_count, 1, 1, 1
    )
    weights = stick_weights(scores, visible).astype(jnp.bfloat16)
    blended = jnp.einsum(
        "bgql,bgld->bgqd", weights, cached_values, preferred_element_type=jnp.float32
    )
    rescale = lax.rsqrt(jnp.mean(blended * blended, axis=3, keepdims=True) + 1e-06)
    normed = ((blended * rescale).reshape(seq_count, local_heads * head_dim) * head_gain).astype(
        jnp.bfloat16
    )
    partial_out = jnp.dot(normed, w_output, preferred_element_type=jnp.float32)
    attended = lax.psum(partial_out.astype(jnp.bfloat16), "tp").astype(jnp.float32)
    settled = layer_norm(
        RESIDUAL_SCALE * tokens.astype(jnp.float32) + attended, attn_norm_gain
    ).astype(jnp.bfloat16)
    experts = w_router.shape[1]
    top_count = routes.shape[1]
    logits = jnp.dot(settled, w_router, preferred_element_type=jnp.float32)
    chosen = routes[:, :, None] == lax.broadcasted_iota(
        jnp.int32, (seq_count, top_count, experts), 2
    )
    picked = jnp.sum(jnp.where(chosen, logits[:, None, :], 0.0), axis=2)
    route_weight = jax.nn.sigmoid(picked - picked[:, ::-1])
    assigned = chosen.reshape(seq_count * top_count, experts).astype(jnp.int32)
    before = jnp.cumsum(assigned, axis=0) - assigned
    slot_index = jnp.sum(before * assigned, axis=1)
    slot_hits = (
        slot_index[:, None] == lax.broadcasted_iota(jnp.int32, (seq_count * top_count, CAP), 1)
    ).astype(jnp.int32)
    placement = (assigned[:, :, None] * slot_hits[:, None, :]).reshape(
        seq_count, top_count, experts * CAP
    )
    selector = jnp.sum(placement, axis=1).astype(jnp.bfloat16)
    weighted = jnp.sum(placement.astype(jnp.float32) * route_weight[:, :, None], axis=1)
    buffer = lax.dot_general(
        selector, settled, (((0,), (0,)), ((), ())), preferred_element_type=jnp.float32
    )
    buffer = buffer.astype(jnp.bfloat16).reshape(experts, CAP, model_width)
    hosts = lax.axis_size("ep")
    tp_size = lax.axis_size("tp")
    if experts >= hosts:
        per_host = experts // hosts
        outgoing = buffer.reshape(hosts, per_host, CAP, model_width)
    else:
        per_host = 1
        outgoing = jnp.repeat(buffer, hosts // experts, axis=0).reshape(hosts, 1, CAP, model_width)
    columns = expert_gate.shape[1]
    block_index = lax.axis_index(("ep", "tp"))
    own_expert = block_index * columns // FE
    local_slot = own_expert - lax.axis_index("ep") * experts // hosts
    slice_width = model_width // tp_size
    arrived = lax.all_to_all(outgoing, "ep", split_axis=0, concat_axis=0, tiled=True)
    slot_count = arrived.shape[2]
    received = lax.dynamic_index_in_dim(arrived, local_slot, 1, keepdims=False)
    received = received.reshape(hosts * slot_count, model_width)
    gate_pre = jnp.dot(received, expert_gate, preferred_element_type=jnp.float32)
    up_pre = jnp.dot(received, expert_up, preferred_element_type=jnp.float32)
    hidden = (jax.nn.silu(gate_pre) * up_pre).astype(jnp.bfloat16)
    partial_value = jnp.dot(hidden, expert_down, preferred_element_type=jnp.float32)
    partial_value = partial_value.reshape(hosts, 1, slot_count, model_width)
    slot_mask = (lax.broadcasted_iota(jnp.int32, (1, per_host, 1, 1), 1) == local_slot).astype(
        jnp.float32
    )
    summed = lax.psum_scatter(
        (partial_value * slot_mask).astype(jnp.bfloat16), "tp", scatter_dimension=3, tiled=True
    ).astype(jnp.float32)
    returned = lax.all_to_all(
        summed.astype(jnp.bfloat16), "ep", split_axis=0, concat_axis=0, tiled=True
    ).astype(summed.dtype)
    host_ids = lax.broadcasted_iota(jnp.int32, (hosts * per_host,), 0)
    host_expert = host_ids // per_host * experts // hosts + host_ids % per_host
    ownership = (
        host_expert[None, :] == lax.broadcasted_iota(jnp.int32, (experts, hosts * per_host), 0)
    ).astype(jnp.float32)
    gathered = jnp.dot(
        ownership, returned.reshape(hosts * per_host, CAP * slice_width), precision=PRECISE
    )
    gathered = gathered.reshape(experts * CAP, slice_width)
    routed = jnp.dot(weighted, gathered, precision=PRECISE)
    column_rank = lax.axis_index("tp")
    own_settled = lax.dynamic_slice_in_dim(settled, column_rank * slice_width, slice_width, 1)
    shard_rows = lax.all_gather(settled, "ep", axis=0, tiled=True)
    gate_pre = jnp.dot(shard_rows, dense_gate, preferred_element_type=jnp.float32)
    up_pre = jnp.dot(shard_rows, dense_up, preferred_element_type=jnp.float32)
    dense_hidden = (jax.nn.silu(gate_pre) * up_pre).astype(jnp.bfloat16)
    own_hidden = lax.all_to_all(dense_hidden, "ep", split_axis=0, concat_axis=1, tiled=True)
    dense_out = jnp.dot(
        own_hidden,
        lax.all_gather(dense_down, "ep", axis=0, tiled=True),
        preferred_element_type=jnp.float32,
    )
    mix_weight = jax.nn.sigmoid(jnp.dot(settled, mix_gate, preferred_element_type=jnp.float32))
    combined = (
        RESIDUAL_SCALE * own_settled.astype(jnp.float32) + routed + mix_weight[:, None] * dense_out
    )
    row_sums, squares = lax.psum(
        (jnp.sum(combined, axis=1), jnp.sum(combined * combined, axis=1)), "tp"
    )
    row_mean = row_sums / model_width
    row_var = squares / model_width - row_mean * row_mean
    result = (
        (combined - row_mean[:, None]) * lax.rsqrt(row_var[:, None] + 1e-05) * ffn_norm_gain
    ).astype(jnp.bfloat16)
    return (result, new_kv)


LANES = 128
HBM_ARGS = (
    "tokens",
    "w_query",
    "kv_cache",
    "w_key",
    "w_value",
    "head_gain",
    "w_output",
    "attn_norm_gain",
    "w_router",
    "mix_gate",
    "expert_gate",
    "expert_up",
    "dense_gate",
    "dense_up",
    "dense_down",
    "expert_down",
    "ffn_norm_gain",
)


EARLY_ARGS = ("tokens", "w_query")
LATE_ARGS = tuple(name for name in HBM_ARGS if name not in EARLY_ARGS + ("kv_cache",))


def silu(values):
    return values / (1.0 + jnp.exp(-values))


def dot_rows(left, right):
    return lax.dot_general(
        left, right, (((1,), (1,)), ((), ())), preferred_element_type=jnp.float32
    )


def layer_kernel(sizes, *refs):
    ep, tp = sizes
    count = len(HBM_ARGS)
    scalars_hbm = refs[:3]
    hbm = dict(zip(HBM_ARGS, refs[3 : 3 + count]))
    out_ref, new_kv_ref = refs[3 + count : 5 + count]
    vmem = dict(zip(HBM_ARGS, refs[5 + count : 5 + 2 * count]))
    (
        parts,
        rows,
        mixes,
        stacked,
        hidden,
        outgoing,
        incoming,
        stats,
        lengths_ref,
        bias_ref,
        routes_ref,
        scalar_sem,
        load_sem,
        kv_sem,
        part_send,
        part_recv,
        row_send,
        row_recv,
        mix_send,
        mix_recv,
        block_send,
        block_recv,
        stat_send,
        stat_recv,
    ) = refs[5 + 2 * count :]
    e = lax.axis_index("ep")
    t = lax.axis_index("tp")
    seqs, width = vmem["tokens"].shape
    positions, kv_width = vmem["kv_cache"].shape[1:]
    head_dim = kv_width // 2
    experts = vmem["w_router"].shape[0]
    columns = vmem["expert_gate"].shape[1]
    slice_width = width // tp
    devices = ep * tp
    me = e * tp + t

    barrier = pltpu.get_barrier_semaphore()

    def greet(k, carry):
        peer = lax.rem(me + k, devices)
        pl.semaphore_signal(
            barrier,
            inc=1,
            device_id=(peer // tp, lax.rem(peer, tp)),
            device_id_type=pl.DeviceIdType.MESH,
        )
        return carry

    def load(name):
        return pltpu.make_async_copy(hbm[name], vmem[name], load_sem.at[HBM_ARGS.index(name)])

    def load_kv(b):
        return pltpu.make_async_copy(
            hbm["kv_cache"].at[b, 0], vmem["kv_cache"].at[b], kv_sem.at[b]
        )

    scalar_loads = [
        pltpu.make_async_copy(source, target, scalar_sem.at[i])
        for i, (source, target) in enumerate(
            zip(scalars_hbm, (lengths_ref, bias_ref, routes_ref))
        )
    ]
    for name in EARLY_ARGS:
        load(name).start()
    for b in range(seqs):
        load_kv(b).start()
    for copy in scalar_loads:
        copy.start()
    lax.fori_loop(1, devices, greet, 0)

    load("tokens").wait()
    load("w_query").wait()
    tokens = vmem["tokens"][...]
    queries = jnp.dot(tokens, vmem["w_query"][...], preferred_element_type=jnp.float32)
    queries = queries.astype(jnp.bfloat16).astype(jnp.float32)
    lane = lax.broadcasted_iota(jnp.int32, (1, kv_width), 1)
    stack = jnp.concatenate([queries, pltpu.roll(queries, head_dim, 1)], axis=0)
    stack = jnp.where(lane < head_dim, stack, 0.0)
    pairs = stack.shape[0]
    row = lax.broadcasted_iota(jnp.int32, (pairs, 1), 0)
    owner = lax.rem(row, seqs)
    scores = jnp.zeros((pairs, positions), jnp.float32)
    for b in range(seqs):
        load_kv(b).wait()
        own = jnp.where(owner == b, stack, 0.0).astype(jnp.bfloat16)
        scores += dot_rows(own, vmem["kv_cache"][b])
    for name in LATE_ARGS:
        load(name).start()
    for copy in scalar_loads:
        copy.wait()
    limit = jnp.zeros((pairs, 1), jnp.int32)
    for b in range(seqs):
        limit = jnp.where(owner == b, lengths_ref[b], limit)
    bias = jnp.where(row < seqs, bias_ref[0], bias_ref[1])
    z = scores * head_dim ** (-0.5) + bias
    visible = lax.broadcasted_iota(jnp.int32, (pairs, positions), 1) < limit
    tail = jnp.log1p(jnp.exp(-jnp.abs(z)))
    survive = jnp.where(visible, -(jnp.maximum(z, 0.0) + tail), 0.0)
    blocks = positions // LANES
    tall = jnp.concatenate(
        [survive[:, j * LANES : (j + 1) * LANES] for j in range(blocks)], axis=0
    )
    high = tall.astype(jnp.bfloat16)
    rest = tall - high.astype(jnp.float32)
    middle = rest.astype(jnp.bfloat16)
    low = (rest - middle.astype(jnp.float32)).astype(jnp.bfloat16)
    later = (
        lax.broadcasted_iota(jnp.int32, (LANES, LANES), 0)
        > lax.broadcasted_iota(jnp.int32, (LANES, LANES), 1)
    ).astype(jnp.float32).astype(jnp.bfloat16)
    sums = jnp.dot(
        jnp.concatenate([high, middle, low], axis=0), later, preferred_element_type=jnp.float32
    )
    height = blocks * pairs
    sums = sums[:height] + sums[height : 2 * height] + sums[2 * height :]
    totals = jnp.sum(tall, axis=1, keepdims=True)
    running = jnp.zeros((pairs, 1), jnp.float32)
    pieces = [None] * blocks
    for j in reversed(range(blocks)):
        pieces[j] = sums[j * pairs : (j + 1) * pairs] + running
        running = running + totals[j * pairs : (j + 1) * pairs]
    remaining = jnp.concatenate(pieces, axis=1)
    weights = jnp.where(visible, jnp.exp(jnp.minimum(z, 0.0) - tail + remaining), 0.0)
    blended = jnp.zeros((pairs, kv_width), jnp.float32)
    for b in range(seqs):
        own = jnp.where(owner == b, weights, 0.0).astype(jnp.bfloat16)
        blended += jnp.dot(own, vmem["kv_cache"][b], preferred_element_type=jnp.float32)
    blended = jnp.where(lane >= head_dim, blended, 0.0)
    spread = jnp.sum(blended * blended, axis=1, keepdims=True) / head_dim
    blended = blended * lax.rsqrt(spread + 1e-06)
    load("head_gain").wait()
    normed = pltpu.roll(blended[:seqs], head_dim, 1) + blended[seqs:]
    normed = (normed * vmem["head_gain"][...]).astype(jnp.bfloat16)
    load("w_output").wait()
    partial = jnp.dot(normed, vmem["w_output"][...], preferred_element_type=jnp.float32)
    parts[t] = partial.astype(jnp.bfloat16)

    pl.semaphore_wait(barrier, devices - 1)

    def to_tp(buffer, send, recv, peer, slot):
        return pltpu.make_async_remote_copy(
            src_ref=buffer.at[slot],
            dst_ref=buffer.at[slot],
            send_sem=send.at[peer],
            recv_sem=recv.at[slot],
            device_id=(e, peer),
            device_id_type=pl.DeviceIdType.MESH,
        )

    def to_ep(buffer, send, recv, peer, slot):
        return pltpu.make_async_remote_copy(
            src_ref=buffer.at[slot],
            dst_ref=buffer.at[slot],
            send_sem=send.at[peer],
            recv_sem=recv.at[slot],
            device_id=(peer, t),
            device_id_type=pl.DeviceIdType.MESH,
        )

    def tp_peer(k):
        return lax.rem(t + k, tp)

    def ep_peer(k):
        return lax.rem(e + k, ep)

    for k in range(1, tp):
        to_tp(parts, part_send, part_recv, tp_peer(k), t).start()

    load("w_key").wait()
    load("w_value").wait()
    key_new = dot_rows(tokens, vmem["w_key"][...])
    value_new = dot_rows(tokens, vmem["w_value"][...])
    new_kv_ref[...] = jnp.concatenate([key_new, value_new], axis=1).astype(jnp.bfloat16)

    load("attn_norm_gain").wait()
    for k in range(1, tp):
        to_tp(parts, part_send, part_recv, tp_peer(k), tp_peer(k)).wait_recv()
    attended = jnp.sum(parts[...].astype(jnp.float32), axis=0)
    settled = layer_norm(
        RESIDUAL_SCALE * tokens.astype(jnp.float32) + attended, vmem["attn_norm_gain"][...]
    ).astype(jnp.bfloat16)
    rows[e] = settled
    for k in range(1, ep):
        to_ep(rows, row_send, row_recv, ep_peer(k), e).start()

    load("w_router").wait()
    load("mix_gate").wait()
    logits = dot_rows(settled, vmem["w_router"][...])
    expert_lane = lax.broadcasted_iota(jnp.int32, (seqs, experts), 1)
    seq_row = lax.broadcasted_iota(jnp.int32, (seqs, 1), 0)
    first = jnp.zeros((seqs, 1), jnp.int32)
    second = jnp.zeros((seqs, 1), jnp.int32)
    for b in range(seqs):
        first = jnp.where(seq_row == b, routes_ref[0, b], first)
        second = jnp.where(seq_row == b, routes_ref[1, b], second)
    first_logit = jnp.sum(jnp.where(expert_lane == first, logits, 0.0), axis=1, keepdims=True)
    second_logit = jnp.sum(jnp.where(expert_lane == second, logits, 0.0), axis=1, keepdims=True)
    settled_wide = settled.astype(jnp.float32)
    mix_gate = vmem["mix_gate"][...].astype(jnp.float32)
    products = jnp.zeros((seqs, LANES), jnp.float32)
    for j in range(width // LANES):
        products += settled_wide[:, j * LANES : (j + 1) * LANES] * mix_gate[j : j + 1]
    mix = jax.nn.sigmoid(jnp.sum(products, axis=1, keepdims=True))
    wide_lane = lax.broadcasted_iota(jnp.int32, (seqs, LANES), 1)
    mixes[e] = (
        jnp.where(wide_lane == first, jax.nn.sigmoid(first_logit - second_logit), 0.0)
        + jnp.where(wide_lane == second, jax.nn.sigmoid(second_logit - first_logit), 0.0)
        + jnp.where(wide_lane == experts, mix, 0.0)
    )
    for k in range(1, ep):
        to_ep(mixes, mix_send, mix_recv, ep_peer(k), e).start()

    for name in ("expert_gate", "expert_up", "dense_gate", "dense_up", "dense_down"):
        load(name).wait()
    for k in range(1, ep):
        to_ep(rows, row_send, row_recv, ep_peer(k), ep_peer(k)).wait_recv()
    stacked[...] = jnp.concatenate(
        [rows[i].astype(jnp.float32) for i in range(ep)], axis=0
    ).astype(jnp.bfloat16)

    tile = 256 if columns % 256 == 0 else LANES

    def up_tile(i, carry):
        at = pl.ds(pl.multiple_of(i * tile, tile), tile)
        gate_pre = jnp.dot(
            stacked[...], vmem["expert_gate"][:, at], preferred_element_type=jnp.float32
        )
        up_pre = jnp.dot(
            stacked[...], vmem["expert_up"][:, at], preferred_element_type=jnp.float32
        )
        hidden[:, at] = (silu(gate_pre) * up_pre).astype(jnp.bfloat16)
        return carry

    lax.fori_loop(0, columns // tile, up_tile, 0)
    gate_pre = dot_rows(stacked[...], vmem["dense_gate"][...])
    up_pre = dot_rows(stacked[...], vmem["dense_up"][...])
    dense_hidden = (silu(gate_pre) * up_pre).astype(jnp.bfloat16)
    dense = jnp.dot(dense_hidden, vmem["dense_down"][...], preferred_element_type=jnp.float32)

    for k in range(1, ep):
        to_ep(mixes, mix_send, mix_recv, ep_peer(k), ep_peer(k)).wait_recv()
    table = mixes[...].reshape(ep * seqs, LANES)
    own_expert = me * experts // devices
    all_lane = lax.broadcasted_iota(jnp.int32, (ep * seqs, LANES), 1)
    expert_weight = jnp.sum(jnp.where(all_lane == own_expert, table, 0.0), axis=1, keepdims=True)
    dense_weight = jnp.sum(jnp.where(all_lane == experts, table, 0.0), axis=1, keepdims=True)
    dense = dense * dense_weight

    def block_copy(source, target, send_slot, recv_slot, to_e, to_t):
        return pltpu.make_async_remote_copy(
            src_ref=outgoing.at[source],
            dst_ref=incoming.at[target],
            send_sem=block_send.at[send_slot],
            recv_sem=block_recv.at[recv_slot],
            device_id=(to_e, to_t),
            device_id_type=pl.DeviceIdType.MESH,
        )

    load("expert_down").wait()
    for j in range(tp):
        value = jnp.dot(
            hidden[...],
            vmem["expert_down"][:, j * slice_width : (j + 1) * slice_width],
            preferred_element_type=jnp.float32,
        )
        value = value * expert_weight + jnp.where(t == j, dense, 0.0)
        for i in range(ep):
            outgoing[i * tp + j] = value[i * seqs : (i + 1) * seqs].astype(jnp.bfloat16)

        def send_block(k, carry, j=j):
            to_e = ep_peer(k)
            peer = to_e * tp + j

            @pl.when(peer != me)
            def _():
                block_copy(peer, me, peer, me, to_e, j).start()

            return carry

        lax.fori_loop(0, ep, send_block, 0)
    incoming[me] = outgoing[me]
    load("ffn_norm_gain").wait()

    def wait_block(k, carry):
        peer = lax.rem(me + k, devices)
        block_copy(peer, peer, peer, peer, peer // tp, lax.rem(peer, tp)).wait_recv()
        return carry

    lax.fori_loop(1, devices, wait_block, 0)
    combined = jnp.sum(incoming[...].astype(jnp.float32), axis=0)
    mine = jnp.zeros((seqs, slice_width), jnp.float32)
    for j in range(tp):
        mine = jnp.where(t == j, settled_wide[:, j * slice_width : (j + 1) * slice_width], mine)
    combined = combined + RESIDUAL_SCALE * mine
    row_sum = jnp.sum(combined, axis=1, keepdims=True)
    square = jnp.sum(combined * combined, axis=1, keepdims=True)
    stats[t] = jnp.where(wide_lane == 0, row_sum, jnp.where(wide_lane == 1, square, 0.0))
    for k in range(1, tp):
        to_tp(stats, stat_send, stat_recv, tp_peer(k), t).start()
    for k in range(1, tp):
        to_tp(stats, stat_send, stat_recv, tp_peer(k), tp_peer(k)).wait_recv()
    both = jnp.sum(stats[...], axis=0)
    row_mean = both[:, :1] / width
    row_var = both[:, 1:2] / width - row_mean * row_mean
    out_ref[...] = (
        (combined - row_mean) * lax.rsqrt(row_var + 1e-05) * vmem["ffn_norm_gain"][...]
    ).astype(jnp.bfloat16)

    for k in range(1, tp):
        to_tp(parts, part_send, part_recv, tp_peer(k), t).wait_send()
        to_tp(stats, stat_send, stat_recv, tp_peer(k), t).wait_send()
    for k in range(1, ep):
        to_ep(rows, row_send, row_recv, ep_peer(k), e).wait_send()
        to_ep(mixes, mix_send, mix_recv, ep_peer(k), e).wait_send()

    def drain(k, carry):
        peer = lax.rem(me + k, devices)
        block_copy(peer, me, peer, me, peer // tp, lax.rem(peer, tp)).wait_send()
        return carry

    lax.fori_loop(1, devices, drain, 0)


def finish_kernel(result_ref, new_kv_ref, result_out, new_kv_out):
    result_out[...] = result_ref[...]
    new_kv_out[...] = new_kv_ref[...]


NAMES = (
    "tokens",
    "kv_cache",
    "lengths",
    "w_query",
    "w_key",
    "w_value",
    "break_bias",
    "head_gain",
    "w_output",
    "attn_norm_gain",
    "w_router",
    "routes",
    "expert_gate",
    "expert_up",
    "expert_down",
    "dense_gate",
    "dense_up",
    "dense_down",
    "mix_gate",
    "ffn_norm_gain",
)


def fused_fits(args, ep, tp):
    seqs, width = args["tokens"].shape
    _, key_heads, positions, kv_width = args["kv_cache"].shape
    experts = args["w_router"].shape[1]
    return (
        seqs == 8
        and key_heads == 1
        and kv_width == LANES
        and args["w_query"].shape[1] == LANES
        and positions % LANES == 0
        and experts < LANES
        and args["routes"].shape[1] == 2
        and (ep * tp) % experts == 0
        and args["expert_gate"].shape[1] % LANES == 0
        and (width // tp) % LANES == 0
    )


def fused(args, ep, tp):
    for name in ("head_gain", "attn_norm_gain", "ffn_norm_gain"):
        args[name] = args[name].reshape(1, -1)
    args["mix_gate"] = args["mix_gate"].reshape(-1, LANES)
    for name in ("w_key", "w_value", "w_router", "routes", "dense_gate", "dense_up"):
        args[name] = args[name].T
    operands = [args[name] for name in HBM_ARGS]
    seqs, width = args["tokens"].shape
    slice_width = width // tp
    devices = ep * tp
    scratch = []
    for name, operand in zip(HBM_ARGS, operands):
        shape = operand.shape
        if name == "kv_cache":
            shape = (shape[0],) + shape[2:]
        scratch.append(pltpu.VMEM(shape, operand.dtype))
    dma = pltpu.SemaphoreType.DMA
    scratch += [
        pltpu.VMEM((tp, seqs, width), jnp.bfloat16),
        pltpu.VMEM((ep, seqs, width), jnp.bfloat16),
        pltpu.VMEM((ep, seqs, LANES), jnp.float32),
        pltpu.VMEM((ep * seqs, width), jnp.bfloat16),
        pltpu.VMEM((ep * seqs, args["expert_gate"].shape[1]), jnp.bfloat16),
        pltpu.VMEM((devices, seqs, slice_width), jnp.bfloat16),
        pltpu.VMEM((devices, seqs, slice_width), jnp.bfloat16),
        pltpu.VMEM((tp, seqs, LANES), jnp.float32),
        pltpu.SMEM(args["lengths"].shape, jnp.int32),
        pltpu.SMEM(args["break_bias"].shape, jnp.float32),
        pltpu.SMEM(args["routes"].shape, jnp.int32),
        dma((3,)),
        dma((len(HBM_ARGS),)),
        dma((seqs,)),
        dma((tp,)),
        dma((tp,)),
        dma((ep,)),
        dma((ep,)),
        dma((ep,)),
        dma((ep,)),
        dma((devices,)),
        dma((devices,)),
        dma((tp,)),
        dma((tp,)),
    ]
    result, new_kv = pl.pallas_call(
        functools.partial(layer_kernel, (ep, tp)),
        out_shape=(
            jax.ShapeDtypeStruct((seqs, slice_width), jnp.bfloat16),
            jax.ShapeDtypeStruct((seqs, LANES), jnp.bfloat16),
        ),
        in_specs=[pl.BlockSpec(memory_space=pl.ANY)] * (3 + len(HBM_ARGS)),
        out_specs=(
            pl.BlockSpec(memory_space=pltpu.VMEM),
            pl.BlockSpec(memory_space=pltpu.VMEM),
        ),
        scratch_shapes=scratch,
        compiler_params=pltpu.CompilerParams(
            collective_id=0, has_side_effects=True, vmem_limit_bytes=60 * 1024 * 1024
        ),
    )(args["lengths"], args["break_bias"], args["routes"], *operands)
    result, new_kv = pl.pallas_call(
        finish_kernel,
        out_shape=(
            jax.ShapeDtypeStruct(result.shape, result.dtype),
            jax.ShapeDtypeStruct(new_kv.shape, new_kv.dtype),
        ),
    )(result, new_kv)
    return result, new_kv.reshape(seqs, 1, LANES)


def layer(ep, tp, *arrays):
    args = dict(zip(NAMES, arrays))
    if fused_fits(args, ep, tp):
        return fused(args, ep, tp)
    return body(*arrays)


def solution(mesh):
    in_specs = (
        P("ep", None),
        P("ep", "tp", None, None),
        P("ep"),
        P(None, "tp"),
        P(None, "tp"),
        P(None, "tp"),
        P("tp"),
        P("tp"),
        P("tp", None),
        P(),
        P(),
        P("ep", None),
        P(None, ("ep", "tp")),
        P(None, ("ep", "tp")),
        P(("ep", "tp"), None),
        P(None, "ep"),
        P(None, "ep"),
        P("ep", "tp"),
        P(),
        P("tp"),
    )
    out_specs = (P("ep", "tp"), P("ep", "tp", None))
    step = functools.partial(layer, mesh.shape["ep"], mesh.shape["tp"])
    return jax.shard_map(step, mesh=mesh, in_specs=in_specs, out_specs=out_specs, check_vma=False)
```
